32 devices in a mesh: sp: 8 (over z, y), tp: 4 (over x, core).
Axes of the slice: x: 2, y: 2, z: 4, core: 2. Of those that a mesh axis runs over, the one named last changes fastest.
Arguments:
- activations: bfloat16 [4096, 2048], P('sp', 'tp'), may hold values from -250 to 250
- norm_gain: bfloat16 [2048], P('tp'), may hold values from 0.099609375 to 1.8984375
- pool_weight: bfloat16 [2048, 1024], P('sp', 'tp'), may hold values from -0.125 to 0.125
- gate_weight: bfloat16 [2048, 1024], P('sp', 'tp'), may hold values from -0.125 to 0.125
- value_weight: bfloat16 [2048, 1024], P('sp', 'tp'), may hold values from -0.125 to 0.125
- key_weight: bfloat16 [2048, 256], P('sp', 'tp'), may hold values from -0.125 to 0.125
- read_weight: bfloat16 [2048, 256], P('sp', 'tp'), may hold values from -0.125 to 0.125
- step_weight: bfloat16 [2048, 16], P('sp', 'tp'), may hold values from -0.125 to 0.125
- pool_mix: bfloat16 [4, 256, 256], P('tp'), may hold values from -0.375 to 0.375
- pool_scale: float32 [1024], P('tp'), may hold values from 0.1 to 1.9
- taps_value: float32 [4, 1024], P(None, 'tp'), may hold values from -3 to 3
- taps_key: float32 [4, 256], P(None, 'tp'), may hold values from -3 to 3
- taps_read: float32 [4, 256], P(None, 'tp'), may hold values from -3 to 3
- step_bias: float32 [16], P('tp'), may hold values from -1 to 1
- decay_log: float32 [16], P('tp')
- decay_extra: float32 [4096, 16], P('sp', 'tp'), may hold values from -1 to 0
- skip_scale: float32 [16], P('tp'), may hold values from 0.5 to 2
- state_gain: float32 [1024], P('tp'), may hold values from 0.1 to 1.9
- out_pool_weight: bfloat16 [1024, 2048], P('tp', 'sp'), may hold values from -0.125 to 0.125
- out_state_weight: bfloat16 [1024, 2048], P('tp', 'sp'), may hold values from -0.125 to 0.125
Outputs:
- mixed: bfloat16 [4096, 2048], P('sp', 'tp')
The draws below stay inside these ranges and needn't reach their ends.
All inputs are finite; a program needn't handle non-finite values.
Results may differ from the reference program's by a relative error of at most 0.007.
Values may be sent and summed in bfloat16 or wider, within the bound.
A program may use at most 64 MiB of HBM per device.

```python
import math
import jax
import jax.numpy as jnp
from jax import lax

D = 2048
SCAN_HEAD_NUMBER = 16
SSM_HEAD_DIM = 64
SSM_GROUPS = 4
SSM_STATE = 64
POOL_GROUPS = 4
MIXER_CONV_TAPS = 4
SCAN_BLOCK = 128
TOK_DEV = 512
MIX_W = 1024
GW = 256
TOKENS = 4096


def draw_activations(key, part):
    first, second = jax.random.split(key, 2)
    spot = jnp.arange(D).astype(jnp.float32) / D
    rough = jnp.exp(jax.random.uniform(second, (1, D), jnp.float32, -0.35, 0.35))
    basic = jnp.clip(jax.random.normal(first, (TOKENS, D), jnp.float32), -4.0, 4.0)
    rising = jnp.exp(spot * 1.1)[None, :]
    return (basic * rising * rough).astype(jnp.bfloat16)


def draw_decay_log(key, part):
    first, second, third = jax.random.split(key, 3)
    fast_rate = jnp.log(jax.random.uniform(first, (SCAN_HEAD_NUMBER,), jnp.float32, 0.03, 0.1))
    slow_rate = jax.random.uniform(second, (SCAN_HEAD_NUMBER,), jnp.float32, jnp.log(0.1), jnp.log(0.5)) - jnp.log(TOKENS * 1.0)
    chance = 0.5
    quick = jax.random.uniform(third, (SCAN_HEAD_NUMBER,), jnp.float32) < chance
    return jnp.where(quick, fast_rate, slow_rate)


def draw_decay_extra(key, part):
    first, second, third, quarter_slice = jax.random.split(key, 4)
    steady_rate = jnp.exp(jax.random.uniform(first, (1, 1, SCAN_HEAD_NUMBER), jnp.float32, jnp.log(0.2), jnp.log(0.6))) / TOKENS
    factor = jnp.exp(jax.random.uniform(second, (TOKENS // TOK_DEV, 1, 1), jnp.float32, jnp.log(0.25), jnp.log(2.0)))
    constant_baseline = -(factor * steady_rate * jnp.ones((1, TOK_DEV, 1), jnp.float32)).reshape(TOKENS, SCAN_HEAD_NUMBER)
    places = jax.random.randint(third, (3,), 0, TOKENS)
    masked_elements = jnp.any(jnp.arange(TOKENS)[:, None] == places[None, :], axis=1)
    sudden_impulse = jnp.log(jax.random.uniform(quarter_slice, (1, SCAN_HEAD_NUMBER), jnp.float32, 0.5, 0.8))
    return constant_baseline + jnp.where(masked_elements[:, None], sudden_impulse, 0.0)


def shard_levels(key, dims, pieces, least, top_value):
    def one(axis_at, blocks):
        steps = jax.random.uniform(jax.random.fold_in(jax.random.fold_in(key, 6), axis_at), (blocks,), jnp.float32, least / len(pieces), top_value / len(pieces))
        return jnp.repeat(jnp.exp(steps), dims[axis_at] // blocks).reshape((-1,) + (1,) * (len(dims) - axis_at - 1))

    gain = one(*pieces[0])
    for cut in pieces[1:]:
        gain = gain * one(*cut)
    return gain


def normal_values(rng, dims, scale, bound, shards=(), held_as=jnp.bfloat16):
    values = scale * jax.random.normal(rng, dims, jnp.float32)
    if shards:
        values = values * shard_levels(rng, dims, shards, -0.22, 0.18)
    return jnp.clip(values, -bound, bound).astype(held_as)


def setup_inputs(seed: int = 0) -> dict:
    streams_of = jax.random.split(jax.random.key(seed), 21)
    activations = draw_activations(jax.random.fold_in(streams_of[20], 71), 0)
    norm_gain = jnp.clip(1.0 + 0.18 * jax.random.normal(streams_of[1], (D,), jnp.float32), 0.099609375, 1.8984375).astype(jnp.bfloat16)
    pool_weight = normal_values(streams_of[2], (D, MIX_W), D ** -0.5, 0.125, ((0, 8), (1, 4)))
    gate_weight = normal_values(streams_of[3], (D, MIX_W), D ** -0.5, 0.125, ((0, 8), (1, 4)))
    value_weight = normal_values(streams_of[4], (D, MIX_W), D ** -0.5, 0.125, ((0, 8), (1, 4)))
    key_weight = normal_values(streams_of[5], (D, SSM_GROUPS * SSM_STATE), D ** -0.5, 0.125, ((0, 8), (1, 4)))
    read_weight = normal_values(streams_of[6], (D, SSM_GROUPS * SSM_STATE), D ** -0.5, 0.125, ((0, 8), (1, 4)))
    step_weight = normal_values(streams_of[7], (D, SCAN_HEAD_NUMBER), D ** -0.5, 0.125, ((0, 8), (1, 4)))
    pool_mix = normal_values(streams_of[8], (POOL_GROUPS, GW, GW), GW ** -0.5, 0.375, ((0, 4),))
    pool_scale = jnp.clip(1.0 + 0.18 * jax.random.normal(streams_of[9], (MIX_W,), jnp.float32), 0.1, 1.9)
    taps_value = normal_values(streams_of[10], (MIXER_CONV_TAPS, MIX_W), MIXER_CONV_TAPS ** -0.5, 3.0, ((1, 4),), jnp.float32)
    taps_key = normal_values(streams_of[11], (MIXER_CONV_TAPS, SSM_GROUPS * SSM_STATE), MIXER_CONV_TAPS ** -0.5, 3.0, ((1, 4),), jnp.float32)
    taps_read = normal_values(streams_of[12], (MIXER_CONV_TAPS, SSM_GROUPS * SSM_STATE), MIXER_CONV_TAPS ** -0.5, 3.0, ((1, 4),), jnp.float32)
    step_bias = jnp.clip(jax.random.uniform(streams_of[13], (SCAN_HEAD_NUMBER,), jnp.float32, -1.0, 1.0) * shard_levels(streams_of[13], (SCAN_HEAD_NUMBER,), ((0, 4),), -0.4, 0.0), -1.0, 1.0)
    decay_log = draw_decay_log(jax.random.fold_in(streams_of[20], 71), 0)
    decay_extra = draw_decay_extra(jax.random.fold_in(streams_of[20], 71), 0)
    skip_scale = jnp.clip(jnp.exp(math.log(2.0) - 1.3862944 * jax.random.uniform(streams_of[16], (SCAN_HEAD_NUMBER,), jnp.float32) ** shard_levels(streams_of[16], (SCAN_HEAD_NUMBER,), ((0, 4),), -0.2, 0.2)), 0.5, 2.0)
    state_gain = jnp.clip(1.0 + 0.18 * jax.random.normal(streams_of[17], (MIX_W,), jnp.float32), 0.1, 1.9)
    out_pool_weight = normal_values(streams_of[18], (MIX_W, D), (2 * MIX_W) ** -0.5, 0.125, ((0, 4), (1, 8)))
    out_state_weight = normal_values(streams_of[19], (MIX_W, D), (2 * MIX_W) ** -0.5, 0.125, ((0, 4), (1, 8)))
    return {"activations": activations, "norm_gain": norm_gain, "pool_weight": pool_weight, "gate_weight": gate_weight, "value_weight": value_weight, "key_weight": key_weight, "read_weight": read_weight, "step_weight": step_weight, "pool_mix": pool_mix, "pool_scale": pool_scale, "taps_value": taps_value, "taps_key": taps_key, "taps_read": taps_read, "step_bias": step_bias, "decay_log": decay_log, "decay_extra": decay_extra, "skip_scale": skip_scale, "state_gain": state_gain, "out_pool_weight": out_pool_weight, "out_state_weight": out_state_weight}


EPSILON = 1e-06
HIGH = lax.Precision.HIGHEST

def backward_kernel(raw, taps):
    width = taps.shape[0]
    length = raw.shape[0]
    padded = jnp.pad(raw.astype(jnp.float32), ((width - 1, 0), (0, 0)))
    total = jnp.zeros(raw.shape, jnp.float32)
    for offset in range(width):
        total = total + taps[offset][None, :] * padded[offset:offset + length]
    return jax.nn.silu(total).astype(jnp.bfloat16)

def scan_block(state, inputs):
    head_value, step_size, log_decay, key_heads, read_heads = inputs
    length = head_value.shape[0]
    running = jnp.cumsum(log_decay, axis=0)
    lower = jnp.arange(length)[:, None] >= jnp.arange(length)[None, :]
    gaps = jnp.where(lower[:, :, None], running[:, None, :] - running[None, :, :], -jnp.inf)
    weights = jnp.einsum('lhn,shn->lsh', read_heads, key_heads, precision=HIGH) * jnp.exp(gaps)
    scaled_value = head_value * step_size[:, :, None]
    inner = jnp.einsum('lsh,shp->lhp', weights, scaled_value, precision=HIGH)
    carried = jnp.einsum('lhn,hpn->lhp', read_heads, state, precision=HIGH) * jnp.exp(running)[:, :, None]
    trailing = jnp.exp(running[-1][None, :] - running)
    fresh = jnp.einsum('shn,sh,shp->hpn', key_heads, trailing, scaled_value, precision=HIGH)
    new_state = state * jnp.exp(running[-1])[:, None, None] + fresh
    return (new_state, inner + carried)

def reference(activations, norm_gain, pool_weight, gate_weight, value_weight, key_weight, read_weight, step_weight, pool_mix, pool_scale, taps_value, taps_key, taps_read, step_bias, decay_log, decay_extra, skip_scale, state_gain, out_pool_weight, out_state_weight):
    values = activations.astype(jnp.float32)
    normed = (values * lax.rsqrt(lax.optimization_barrier(jnp.mean(values * values, axis=-1, keepdims=True)) + EPSILON) * norm_gain.astype(jnp.float32)).astype(jnp.bfloat16)
    pool_in = jnp.dot(normed, pool_weight, preferred_element_type=jnp.float32).astype(jnp.bfloat16)
    gate_in = jnp.dot(normed, gate_weight, preferred_element_type=jnp.float32).astype(jnp.bfloat16)
    raw_value = jnp.dot(normed, value_weight, preferred_element_type=jnp.float32).astype(jnp.bfloat16)
    raw_key = jnp.dot(normed, key_weight, preferred_element_type=jnp.float32).astype(jnp.bfloat16)
    raw_read = jnp.dot(normed, read_weight, preferred_element_type=jnp.float32).astype(jnp.bfloat16)
    step_raw = jnp.dot(normed, step_weight, preferred_element_type=jnp.float32)
    reach = 2 ** POOL_GROUPS - 1
    pool_values = pool_in.astype(jnp.float32)
    padded = jnp.pad(pool_values, ((reach, 0), (0, 0)))
    position = jnp.arange(TOKENS).astype(jnp.float32)
    outputs = []
    for group in range(POOL_GROUPS):
        window = 2 ** (group + 1)
        column_count = padded[:, group * GW:(group + 1) * GW]
        window_sum = jnp.zeros((TOKENS, GW), jnp.float32)
        for back in range(window):
            window_sum = window_sum + column_count[reach - back:reach - back + TOKENS]
        counts = jnp.minimum(position + 1.0, float(window))
        pooled = (window_sum / counts[:, None] - pool_values[:, group * GW:(group + 1) * GW]).astype(jnp.bfloat16)
        outputs.append(jnp.dot(pooled, pool_mix[group], preferred_element_type=jnp.float32))
    pool_out = (jnp.concatenate(outputs, axis=1) * pool_scale).astype(jnp.bfloat16)
    head_value = backward_kernel(raw_value, taps_value)
    key_vectors = backward_kernel(raw_key, taps_key)
    read_vectors = backward_kernel(raw_read, taps_read)
    step_size = jax.nn.softplus(step_raw + step_bias)
    log_decay = -jnp.exp(decay_log) * step_size + decay_extra
    repeat = SCAN_HEAD_NUMBER // SSM_GROUPS
    blocks = TOKENS // SCAN_BLOCK
    value_heads = head_value.astype(jnp.float32).reshape(TOKENS, SCAN_HEAD_NUMBER, SSM_HEAD_DIM)
    key_heads = jnp.repeat(key_vectors.astype(jnp.float32).reshape(TOKENS, SSM_GROUPS, SSM_STATE), repeat, axis=1)
    read_heads = jnp.repeat(read_vectors.astype(jnp.float32).reshape(TOKENS, SSM_GROUPS, SSM_STATE), repeat, axis=1)
    start = jnp.zeros((SCAN_HEAD_NUMBER, SSM_HEAD_DIM, SSM_STATE), jnp.float32)
    _, scanned = lax.scan(scan_block, start, (value_heads.reshape(blocks, SCAN_BLOCK, SCAN_HEAD_NUMBER, SSM_HEAD_DIM), step_size.reshape(blocks, SCAN_BLOCK, SCAN_HEAD_NUMBER), log_decay.reshape(blocks, SCAN_BLOCK, SCAN_HEAD_NUMBER), key_heads.reshape(blocks, SCAN_BLOCK, SCAN_HEAD_NUMBER, SSM_STATE), read_heads.reshape(blocks, SCAN_BLOCK, SCAN_HEAD_NUMBER, SSM_STATE)))
    scan_out = scanned.reshape(TOKENS, SCAN_HEAD_NUMBER, SSM_HEAD_DIM) + skip_scale[None, :, None] * value_heads
    gated = scan_out.reshape(TOKENS, MIX_W) * jax.nn.silu(gate_in.astype(jnp.float32))
    state_out = (gated * lax.rsqrt(lax.optimization_barrier(jnp.mean(gated * gated, axis=-1, keepdims=True)) + EPSILON) * state_gain).astype(jnp.bfloat16)
    result = jnp.dot(pool_out, out_pool_weight, preferred_element_type=jnp.float32) + jnp.dot(state_out, out_state_weight, preferred_element_type=jnp.float32)
    return result.astype(jnp.bfloat16)
```

```python
import functools

import jax
import jax.numpy as jnp
from jax import lax
from jax.experimental import pallas as pl
from jax.experimental.pallas import tpu as pltpu
from jax.sharding import PartitionSpec as P

SSM_STATE = 64
POOL_GROUPS = 4
SCAN_BLOCK = 128
MIX_W = 1024


EPSILON = 1e-06
HIGH = lax.Precision.HIGHEST


def shifted(value, axis, steps):
    count = lax.axis_size(axis)
    leading, last = (max(0, -steps), min(count, count - steps))
    return lax.ppermute(value, axis, [(source, source + steps) for source in range(leading, last)])


def carried_in(part, axis, combine, identity):
    place = lax.axis_index(axis)
    gathered = jax.tree.map(lambda a: lax.all_gather(a, axis), part)
    state = jax.tree.map(lambda a, e: jnp.zeros_like(a) + jnp.asarray(e, a.dtype), part, identity)

    def one(step, state):
        return combine(
            state, jax.tree.map(lambda a: lax.dynamic_index_in_dim(a, step, 0, False), gathered)
        )

    return lax.fori_loop(0, place, one, state)


def backward_kernel(extended, taps):
    width = taps.shape[0]
    length = extended.shape[0] - (width - 1)
    widened_rows = extended.astype(jnp.float32)
    total = jnp.zeros((length, extended.shape[1]), jnp.float32)
    for offset in range(width):
        total = total + taps[offset][None, :] * widened_rows[offset : offset + length]
    return jax.nn.silu(total).astype(jnp.bfloat16)


def combine_states(preceding_token, later):
    return (preceding_token[0] * later[0], preceding_token[1] * later[0][:, None, None] + later[1])


def local(
    activations,
    norm_gain,
    pool_weight,
    gate_weight,
    value_weight,
    key_weight,
    read_weight,
    step_weight,
    pool_mix,
    pool_scale,
    taps_value,
    taps_key,
    taps_read,
    step_bias,
    decay_log,
    decay_extra,
    skip_scale,
    state_gain,
    out_pool_weight,
    out_state_weight,
):
    length = activations.shape[0]
    cluster_span = pool_weight.shape[1]
    local_mix = gate_weight.shape[1]
    local_state = key_weight.shape[1]
    local_heads = step_weight.shape[1]
    joined = jnp.concatenate(
        [pool_weight, gate_weight, value_weight, key_weight, read_weight, step_weight], axis=1
    )
    in_weight = lax.all_gather(joined, "sp", axis=0, tiled=True)
    whole, gains = (
        lax.all_gather(activations, "tp", axis=1, tiled=True),
        lax.all_gather(norm_gain, "tp", axis=0, tiled=True),
    )
    widened_rows = whole.astype(jnp.float32)
    normed = (
        widened_rows
        * lax.rsqrt(jnp.mean(widened_rows * widened_rows, axis=-1, keepdims=True) + EPSILON)
        * gains.astype(jnp.float32)
    ).astype(jnp.bfloat16)
    projected = jnp.dot(normed, in_weight, preferred_element_type=jnp.float32)
    column = 0
    pool_in = projected[:, column : column + cluster_span].astype(jnp.bfloat16)
    column = column + cluster_span
    gate_in = projected[:, column : column + local_mix].astype(jnp.bfloat16)
    column = column + local_mix
    raw_value = projected[:, column : column + local_mix].astype(jnp.bfloat16)
    column = column + local_mix
    raw_key = projected[:, column : column + local_state].astype(jnp.bfloat16)
    column = column + local_state
    raw_read = projected[:, column : column + local_state].astype(jnp.bfloat16)
    column = column + local_state
    step_raw = projected[:, column : column + local_heads]
    raw_joined = jnp.concatenate([raw_value, raw_key, raw_read], axis=1)
    reach = 2**POOL_GROUPS - 1
    width = taps_value.shape[0]
    prior_pool, prior_joined = shifted(
        (pool_in[length - reach :], raw_joined[length - width + 1 :]), "sp", 1
    )
    group = lax.axis_index("tp")
    running = jnp.concatenate([prior_pool, pool_in], axis=0).astype(jnp.float32)
    levels = []
    for level in range(POOL_GROUPS):
        stride = 2**level
        running = running[stride:] + running[:-stride]
        levels.append(running[running.shape[0] - length :])
    window_sum = lax.dynamic_index_in_dim(jnp.stack(levels), group, 0, keepdims=False)
    window = jnp.exp2((group + 1).astype(jnp.float32))
    position = (lax.axis_index("sp") * length + jnp.arange(length, dtype=jnp.int32)).astype(
        jnp.float32
    )
    counts = jnp.minimum(position + 1.0, window)
    pooled = (window_sum / counts[:, None] - pool_in.astype(jnp.float32)).astype(jnp.bfloat16)
    pool_out = (
        jnp.dot(pooled, pool_mix[0], preferred_element_type=jnp.float32) * pool_scale
    ).astype(jnp.bfloat16)
    all_taps = jnp.concatenate([taps_value, taps_key, taps_read], axis=1)
    convolved = backward_kernel(jnp.concatenate([prior_joined, raw_joined], axis=0), all_taps)
    head_value = convolved[:, :local_mix]
    key_vectors = convolved[:, local_mix : local_mix + local_state]
    read_vectors = convolved[:, local_mix + local_state :]
    head_dim = local_mix // local_heads
    groups_here = local_state // SSM_STATE
    repeat = local_heads // groups_here
    blocks = length // SCAN_BLOCK
    step_size = jax.nn.softplus(step_raw + step_bias)
    log_decay = -jnp.exp(decay_log) * step_size + decay_extra
    value_heads = head_value.astype(jnp.float32).reshape(length, local_heads, head_dim)
    value_blocks = value_heads.reshape(blocks, SCAN_BLOCK, local_heads, head_dim)
    key_blocks = jnp.repeat(
        key_vectors.astype(jnp.float32).reshape(length, groups_here, SSM_STATE), repeat, axis=1
    ).reshape(blocks, SCAN_BLOCK, local_heads, SSM_STATE)
    read_blocks = jnp.repeat(
        read_vectors.astype(jnp.float32).reshape(length, groups_here, SSM_STATE), repeat, axis=1
    ).reshape(blocks, SCAN_BLOCK, local_heads, SSM_STATE)
    step_blocks = step_size.reshape(blocks, SCAN_BLOCK, local_heads)
    running_decay = jnp.cumsum(log_decay.reshape(blocks, SCAN_BLOCK, local_heads), axis=1)
    lower = jnp.arange(SCAN_BLOCK)[:, None] >= jnp.arange(SCAN_BLOCK)[None, :]
    gaps = jnp.where(
        lower[None, :, :, None],
        running_decay[:, :, None, :] - running_decay[:, None, :, :],
        -jnp.inf,
    )
    weights = jnp.einsum("blhn,bshn->blsh", read_blocks, key_blocks, precision=HIGH) * jnp.exp(gaps)
    scaled_value = value_blocks * step_blocks[..., None]
    inner = jnp.einsum("blsh,bshp->blhp", weights, scaled_value, precision=HIGH)
    block_ends = running_decay[:, -1, :]
    trailing = jnp.exp(block_ends[:, None, :] - running_decay)
    fresh = jnp.einsum("bshn,bsh,bshp->bhpn", key_blocks, trailing, scaled_value, precision=HIGH)

    def advance(carry, inputs):
        block_decay, block_state = inputs
        return (carry * block_decay[:, None, None] + block_state, carry)

    local_total, prefix = lax.scan(
        advance,
        jnp.zeros((local_heads, head_dim, SSM_STATE), jnp.float32),
        (jnp.exp(block_ends), fresh),
    )
    offsets = jnp.cumsum(block_ends, axis=0) - block_ends
    device_decay = jnp.exp(offsets[-1] + block_ends[-1])
    incoming_decay, incoming = carried_in(
        (device_decay, local_total),
        "sp",
        combine_states,
        (jnp.ones_like(device_decay), jnp.zeros_like(local_total)),
    )
    from_device = running_decay + offsets[:, None, :]
    local_off = (
        jnp.einsum("blhn,bhpn->blhp", read_blocks, prefix, precision=HIGH)
        * jnp.exp(running_decay)[..., None]
    )
    far_off = (
        jnp.einsum("blhn,hpn->blhp", read_blocks, incoming, precision=HIGH)
        * jnp.exp(from_device)[..., None]
    )
    scan_out = (inner + local_off + far_off).reshape(length, local_heads, head_dim) + skip_scale[
        None, :, None
    ] * value_heads
    gated = scan_out.reshape(length, local_mix) * jax.nn.silu(gate_in.astype(jnp.float32))
    gate_squares = lax.psum(jnp.sum(gated * gated, axis=-1), "tp")
    state_out = (gated * lax.rsqrt(gate_squares / MIX_W + EPSILON)[:, None] * state_gain).astype(
        jnp.bfloat16
    )
    branch_rows = jnp.concatenate([pool_out, state_out], axis=1)
    out_weight = jnp.concatenate([out_pool_weight, out_state_weight], axis=0)
    terms = jnp.dot(
        branch_rows,
        lax.all_gather(out_weight, "sp", axis=1, tiled=True),
        preferred_element_type=jnp.float32,
    )
    result = lax.psum_scatter(terms, "tp", scatter_dimension=1, tiled=True)
    return result.astype(jnp.bfloat16)


BF = jnp.bfloat16
F32 = jnp.float32
MESH = pl.DeviceIdType.MESH


def flip(index, mask):
    bit = 1
    while bit <= mask:
        if mask & bit:
            index = index + bit - 2 * bit * lax.rem(lax.div(index, bit), 2)
        bit *= 2
    return index


def low_bit(mask):
    return mask & -mask


def spread(size):
    bits = [1 << k for k in reversed(range(size.bit_length() - 1))]
    order, held = [], [0]
    for bit in bits:
        fresh = [mask | bit for mask in held]
        order += fresh
        held += fresh
    return bits, order


def bt(a, b, **kw):
    return lax.dot_general(a, b, (((1,), (1,)), ((), ())), preferred_element_type=F32, **kw)


def halves(x):
    top = x.astype(BF)
    return top, (x - top.astype(F32)).astype(BF)


def mixer_kernel(
    S, T,
    act, gain, pool_w, gate_w, value_w, key_w, read_w, step_t, mix, scale, taps_v, taps_k, taps_r,
    head_par, extra_t, skip, sgain, opool, ostate,
    out,
    wbuf, sbuf, obuf, abuf, nbuf, acc, sacc, ext, conv, hsend, hrecv, scan, xs, xr, ssend, srecv,
    brow, psend, precv, pown, qsend, qrecv, expd,
    w_ss, w_rs, s_ss, s_rs, o_ss, o_rs, a_ss, a_rs, h_ss, h_rs, x_ss, x_rs, q_ss, q_rs, p_ss, p_rs, r_ss, r_rs,
):
    n, da = act.shape
    kd = pool_w.shape[0]
    cw = pool_w.shape[1]
    st = key_w.shape[1]
    ncol = wbuf.shape[2]
    blk = SCAN_BLOCK
    blocks = n // blk
    hd = SSM_STATE
    me = lax.axis_index("sp")
    tp = lax.axis_index("tp")
    sp_bits, sp_order = spread(S)
    tp_bits, tp_order = spread(T)

    wbuf[me, :, 0:cw] = pool_w[...]
    wbuf[me, :, cw : 2 * cw] = gate_w[...]
    wbuf[me, :, 2 * cw : 3 * cw] = value_w[...]
    wbuf[me, :, 3 * cw : 3 * cw + st] = key_w[...]
    wbuf[me, :, 3 * cw + st :] = read_w[...]
    sbuf[me] = step_t[...]
    abuf[tp, 0:n, :] = act[...]
    abuf[tp, n : n + 16, :] = jnp.broadcast_to(gain[...].astype(F32), (16, da)).astype(BF)

    barrier = pltpu.get_barrier_semaphore()
    for k in range(1, S):
        pl.semaphore_signal(barrier, inc=1, device_id={"sp": lax.rem(me + k, S)}, device_id_type=MESH)
    for k in range(1, T):
        pl.semaphore_signal(barrier, inc=1, device_id={"tp": lax.rem(tp + k, T)}, device_id_type=MESH)
    obuf[me, 0:cw, :] = opool[...]
    obuf[me, cw:, :] = ostate[...]
    pl.semaphore_wait(barrier, S - 1 + T - 1)

    started = []

    def remote(src, dst, ss, rs, **peer):
        c = pltpu.make_async_remote_copy(
            src_ref=src, dst_ref=dst, send_sem=ss, recv_sem=rs, device_id=peer, device_id_type=MESH
        )
        return c

    def send(*a, **k):
        c = remote(*a, **k)
        c.start()
        started.append(c)

    def send_block(buf, ss, rs, mask, bit, axis):
        place = me if axis == "sp" else tp
        i = flip(place, mask)
        send(buf.at[i], buf.at[i], ss.at[mask | bit], rs.at[mask | bit], **{axis: flip(place, bit)})

    def arrive(buf, ss, rs, mask, axis):
        place = me if axis == "sp" else tp
        i = flip(place, mask)
        remote(buf.at[i], buf.at[i], ss.at[mask], rs.at[mask], **{axis: flip(place, low_bit(mask))}).wait_recv()

    def push(axis, mask, *trios):
        bits = sp_bits if axis == "sp" else tp_bits
        for bit in bits:
            if mask == 0 or bit < low_bit(mask):
                for buf, ss, rs in trios:
                    send_block(buf, ss, rs, mask, bit, axis)

    W = (wbuf, w_ss, w_rs)
    ST = (sbuf, s_ss, s_rs)
    O = (obuf, o_ss, o_rs)
    A = (abuf, a_ss, a_rs)
    push("tp", 0, A)
    push("sp", 0, W, ST)
    for mask in tp_order:
        arrive(*A, mask, "tp")
        push("tp", mask, A)

    def got(mask):
        arrive(*W, mask, "sp")
        arrive(*ST, mask, "sp")
        push("sp", mask, W, ST)

    got(sp_order[0])
    per = da // kd
    rt = 64

    def norm_rows(i, _):
        r = pl.ds(pl.multiple_of(i * rt, rt), rt)
        parts = [abuf[t, r, :].astype(F32) for t in range(T)]
        tot = sum(jnp.sum(p * p, axis=-1, keepdims=True) for p in parts)
        rs = lax.rsqrt(tot / (da * T) + EPSILON)
        for t in range(T):
            g = abuf[t, n : n + 1, :].astype(F32)
            v = (parts[t] * rs * g).astype(BF)
            for j in range(per):
                nbuf[t * per + j, r, :] = v[:, j * kd : (j + 1) * kd]
        return 0

    lax.fori_loop(0, n // rt, norm_rows, 0)
    mt = 256

    def add_chunk(i, first):
        for r0 in range(0, n, mt):
            x = nbuf[i, r0 : r0 + mt, :]
            d = jnp.dot(x, wbuf[i], preferred_element_type=F32)
            if first:
                acc[r0 : r0 + mt, :] = d
            else:
                acc[r0 : r0 + mt, :] += d
        d = bt(sbuf[i], nbuf[i])
        if first:
            sacc[...] = d
        else:
            sacc[...] += d

    add_chunk(me, True)
    add_chunk(flip(me, sp_order[0]), False)
    for k, mask in enumerate(sp_order[1:]):
        got(mask)
        add_chunk(flip(me, mask), False)
        if mask == sp_order[S // 2 - 2]:
            push("sp", 0, O)

    raw0 = 16
    ccol = ncol - cw
    hsend[:, 0:cw] = acc[n - raw0 :, 0:cw].astype(BF)
    hsend[:, cw:] = acc[n - raw0 :, 2 * cw :].astype(BF)

    def halo():
        return remote(hsend, hrecv, h_ss, h_rs, sp=lax.rem(me + 1, S))

    @pl.when(me < S - 1)
    def _():
        halo().start()

    ext[raw0:, 0:cw] = acc[:, 0:cw].astype(BF).astype(F32)
    ext[raw0:, cw:] = acc[:, 2 * cw :].astype(BF).astype(F32)
    step = sacc[...] + head_par[:, 0:1]
    step = jnp.maximum(step, 0.0) + jnp.log1p(jnp.exp(-jnp.abs(step)))
    ld = head_par[:, 1:2] * step + extra_t[...]
    hp = ld.shape[0]
    r_i = lax.broadcasted_iota(jnp.int32, (blk, blk), 0)
    c_i = lax.broadcasted_iota(jnp.int32, (blk, blk), 1)
    upper = jnp.where(r_i <= c_i, 1.0, 0.0).astype(F32)
    eye = jnp.where(r_i == c_i, 1.0, 0.0).astype(F32)
    lower = r_i >= c_i
    expand = jnp.where(
        lax.broadcasted_iota(jnp.int32, (hp, cw), 1) // hd == lax.broadcasted_iota(jnp.int32, (hp, cw), 0), 1.0, 0.0
    ).astype(F32)
    eye_st = jnp.where(
        lax.broadcasted_iota(jnp.int32, (st, st), 0) == lax.broadcasted_iota(jnp.int32, (st, st), 1), 1.0, 0.0
    ).astype(BF)
    cum_rs, cum_cs, st_rs, wexps = [], [], [], []
    for b in range(blocks):
        cols = slice(b * blk, (b + 1) * blk)
        cum_r = jnp.dot(ld[:, cols], upper, precision=HIGH, preferred_element_type=F32)
        st_r = step[:, cols]
        turned = bt(eye, jnp.concatenate([cum_r, st_r], axis=0), precision=HIGH)
        cum_c = turned[:, 0:hp]
        w_c = jnp.exp(cum_c[blk - 1 : blk, :] - cum_c) * turned[:, hp:]
        both = jnp.dot(
            jnp.concatenate([w_c, jnp.exp(cum_c)], axis=0), expand, precision=HIGH, preferred_element_type=F32
        )
        expd[cols, :] = both[blk:, :]
        wexps.append(both[:blk, :])
        cum_rs.append(cum_r)
        cum_cs.append(cum_c)
        st_rs.append(st_r)

    @pl.when(me > 0)
    def _():
        halo().wait_recv()
        ext[0:raw0, :] = hrecv[...].astype(F32)

    @pl.when(me == 0)
    def _():
        ext[0:raw0, :] = jnp.zeros((raw0, ext.shape[1]), F32)

    width = taps_v.shape[0]
    for b in range(blocks):
        for taps, lo, hi in ((taps_v, 0, cw), (taps_k, cw, cw + st), (taps_r, cw + st, cw + 2 * st)):
            total = jnp.zeros((blk, hi - lo), F32)
            for k in range(width):
                o = b * blk + raw0 - (width - 1) + k
                total = total + taps[k : k + 1, :] * ext[o : o + blk, cw + lo : cw + hi]
            conv[b * blk : (b + 1) * blk, lo:hi] = (total * jax.nn.sigmoid(total)).astype(BF)

    run = jnp.zeros((st, cw), F32)
    dec = jnp.ones((1, cw), F32)
    pres, offs = [], []
    for b in range(blocks):
        rows = slice(b * blk, (b + 1) * blk)
        key_t = bt(eye_st, conv[rows, cw : cw + st]).astype(BF)
        sv = conv[rows, 0:cw].astype(F32) * wexps[b]
        top, low = halves(sv)
        new = jnp.dot(key_t, top, preferred_element_type=F32) + jnp.dot(key_t, low, preferred_element_type=F32)
        bd = expd[(b + 1) * blk - 1 : (b + 1) * blk, :]
        pres.append(run)
        offs.append(dec)
        run = run * bd + new
        dec = dec * bd

    in_s = jnp.zeros((st, cw), F32)
    in_d = jnp.ones((1, cw), F32)
    rounds = [1 << k for k in range(S.bit_length() - 1)]

    def inner(b):
        rows = slice(b * blk, (b + 1) * blk)
        g = bt(conv[rows, cw + st :], conv[rows, cw : cw + st])
        for h in range(cw // hd):
            gap = jnp.where(lower, cum_cs[b][:, h : h + 1] - cum_rs[b][h : h + 1, :], -jnp.inf)
            wm = g * jnp.exp(gap) * st_rs[b][h : h + 1, :]
            top, low = halves(wm)
            v = conv[rows, h * hd : (h + 1) * hd]
            scan[rows, h * hd : (h + 1) * hd] = jnp.dot(top, v, preferred_element_type=F32) + jnp.dot(
                low, v, preferred_element_type=F32
            )

    window = lax.shift_left(jnp.int32(2), tp)
    back = (
        lax.broadcasted_iota(jnp.int32, (blk, blk + raw0), 0)
        + raw0
        - lax.broadcasted_iota(jnp.int32, (blk, blk + raw0), 1)
    )
    band = jnp.where((back >= 0) & (back < window), 1.0, 0.0).astype(BF)

    def pool(b):
        rows = slice(b * blk, (b + 1) * blk)
        sums = jnp.dot(band, ext[b * blk : (b + 1) * blk + raw0, 0:cw].astype(BF), preferred_element_type=F32)
        pos = (me * n + b * blk + lax.broadcasted_iota(jnp.int32, (blk, cw), 0)).astype(F32)
        counts = jnp.minimum(pos + 1.0, window.astype(F32))
        pooled = (sums / counts - ext[b * blk + raw0 : (b + 1) * blk + raw0, 0:cw]).astype(BF)
        brow[rows, 0:cw] = (jnp.dot(pooled, mix[0], preferred_element_type=F32) * scale[...]).astype(BF)

    work = [functools.partial(inner, b) for b in range(blocks)] + [functools.partial(pool, b) for b in range(blocks)]
    share = -(-len(work) // len(rounds))
    o_left = list(sp_order)

    def take_o(count):
        for mask in o_left[:count]:
            arrive(*O, mask, "sp")
            push("sp", mask, O)
        del o_left[:count]

    for r, bit in enumerate(rounds):
        xs[r, 0:st, :] = run
        xs[r, st:, :] = jnp.broadcast_to(dec, (xs.shape[1] - st, cw))
        send(xs.at[r], xr.at[r], x_ss.at[r], x_rs.at[r], sp=flip(me, bit))
        for f in work[r * share : (r + 1) * share]:
            f()
        take_o(1)
        remote(xs.at[r], xr.at[r], x_ss.at[r], x_rs.at[r], sp=flip(me, bit)).wait_recv()
        other, odec = xr[r, 0:st, :], xr[r, st : st + 1, :]
        later = lax.rem(lax.div(me, bit), 2) == 1
        in_s = jnp.where(later, other * in_d + in_s, in_s)
        in_d = jnp.where(later, odec * in_d, in_d)
        run = jnp.where(later, other * dec + run, run * odec + other)
        dec = dec * odec

    for b in range(blocks):
        rows = slice(b * blk, (b + 1) * blk)
        top, low = halves(pres[b] + offs[b] * in_s)
        rd = conv[rows, cw + st :]
        carried = jnp.dot(rd, top, preferred_element_type=F32) + jnp.dot(rd, low, preferred_element_type=F32)
        y = scan[rows, :] + carried * expd[rows, :] + skip[...] * conv[rows, 0:cw].astype(F32)
        gt = acc[rows, cw : 2 * cw].astype(BF).astype(F32)
        gated = y * (gt * jax.nn.sigmoid(gt))
        ssend[:, rows] = bt(jnp.ones((8, cw), F32), gated * gated, precision=HIGH)
        brow[rows, cw:] = (gated * sgain[...]).astype(BF)
    for k in range(1, T):
        send(ssend, srecv.at[k - 1], q_ss.at[k - 1], q_rs.at[k - 1], tp=flip(tp, k))
    take_o(len(o_left))
    for k in range(1, T):
        remote(ssend, srecv.at[k - 1], q_ss.at[k - 1], q_rs.at[k - 1], tp=flip(tp, k)).wait_recv()
    sq = ssend[...]
    for k in range(1, T):
        sq = sq + srecv[k - 1]
    rs_row = lax.rsqrt(sq / (cw * T) + EPSILON)
    rs_cols = [bt(eye, rs_row[:, b * blk : (b + 1) * blk], precision=HIGH)[:, 0:1] for b in range(blocks)]
    wide = S // T
    oc = obuf.shape[2]
    parts = 2
    pr = n // parts

    def product(t, part, store):
        rows = slice(part * pr, (part + 1) * pr)
        rs = jnp.concatenate(rs_cols[part * blocks // parts : (part + 1) * blocks // parts], axis=0)
        for j in range(wide):
            i = t * wide + j
            p = jnp.dot(brow[rows, 0:cw], obuf[i, 0:cw, :], preferred_element_type=F32)
            p = p + rs * jnp.dot(brow[rows, cw:], obuf[i, cw:, :], preferred_element_type=F32)
            store(rows, slice(j * oc, (j + 1) * oc), p)

    def into(ref, *lead):
        def store(rows, cols, p):
            ref[lead + (rows, cols)] = p.astype(ref.dtype)
        return store

    near = flip(tp, 1)

    def near_copy(k, part):
        rows = pl.ds(part * pr, pr)
        i = k * parts + part
        return remote(psend.at[k, rows], precv.at[k, rows], p_ss.at[i], p_rs.at[i], tp=near)

    def far_copy(part):
        rows = pl.ds(part * pr, pr)
        return remote(qsend.at[rows], qrecv.at[rows], r_ss.at[part], r_rs.at[part], tp=flip(tp, 2))

    for part in range(parts):
        product(flip(tp, 3), part, into(psend, 0))
        near_copy(0, part).start()
    for part in range(parts):
        rows = slice(part * pr, (part + 1) * pr)
        product(flip(tp, 2), part, into(pown))
        near_copy(0, part).wait_recv()
        qsend[rows, :] = (pown[rows, :] + precv[0, rows, :]).astype(BF)
        far_copy(part).start()
    for part in range(parts):
        product(near, part, into(psend, 1))
        near_copy(1, part).start()
    for part in range(parts):
        product(tp, part, into(pown))
    for part in range(parts):
        rows = slice(part * pr, (part + 1) * pr)
        near_copy(1, part).wait_recv()
        far_copy(part).wait_recv()
        out[rows, :] = (pown[rows, :] + precv[1, rows, :] + qrecv[rows, :].astype(F32)).astype(out.dtype)

    for c in started:
        c.wait_send()
    for part in range(parts):
        near_copy(0, part).wait_send()
        near_copy(1, part).wait_send()
        far_copy(part).wait_send()

    @pl.when(me < S - 1)
    def _():
        halo().wait_send()


def fits(S, T, shapes):
    n, da = shapes[0]
    kd, cw = shapes[2]
    st = shapes[5][1]
    oc = shapes[18][1]
    heads = shapes[7][1]
    return (
        T == 4 == POOL_GROUPS and S >= T and S & (S - 1) == 0 and S <= 16 and st == SSM_STATE
        and cw == heads * SSM_STATE and oc % 128 == 0 and kd % 128 == 0 and da % kd == 0
        and n % (2 * SCAN_BLOCK) == 0 and cw % 128 == 0 and oc * S == da * T
    )


def fused(
    S, T, activations, norm_gain, pool_weight, gate_weight, value_weight, key_weight, read_weight,
    step_weight, pool_mix, pool_scale, taps_value, taps_key, taps_read, step_bias, decay_log,
    decay_extra, skip_scale, state_gain, out_pool_weight, out_state_weight,
):
    n, da = activations.shape
    kd, cw = pool_weight.shape
    st = key_weight.shape[1]
    heads = step_weight.shape[1]
    oc = out_pool_weight.shape[1]
    hp = 16
    pad = lambda x: jnp.pad(x, ((0, hp - heads), (0, 0)))
    head_par = jnp.pad(jnp.stack([step_bias, -jnp.exp(decay_log)], axis=1), ((0, hp - heads), (0, 126)))
    args = (
        activations, norm_gain[None, :], pool_weight, gate_weight, value_weight, key_weight, read_weight,
        pad(step_weight.T), pool_mix, pool_scale[None, :], taps_value, taps_key, taps_read, head_par,
        pad(decay_extra.T), jnp.repeat(skip_scale, cw // heads)[None, :], state_gain[None, :],
        out_pool_weight, out_state_weight,
    )
    ncol = 3 * cw + 2 * st
    ccol = ncol - cw
    V = pltpu.VMEM
    D = pltpu.SemaphoreType.DMA
    R = S.bit_length() - 1
    scratch = [
        V((S, kd, ncol), BF), V((S, hp, kd), BF), V((S, 2 * cw, oc), BF), V((T, n + 16, da), BF),
        V((S, n, kd), BF), V((n, ncol), F32), V((hp, n), F32), V((n + 16, ccol), F32),
        V((n, cw + 2 * st), BF), V((16, ccol), BF), V((16, ccol), BF), V((n, cw), F32),
        V((R, st + 8, cw), F32), V((R, st + 8, cw), F32), V((8, n), F32), V((T - 1, 8, n), F32),
        V((n, 2 * cw), BF), V((2, n, da), F32), V((2, n, da), F32), V((n, da), F32),
        V((n, da), BF), V((n, da), BF), V((n, cw), F32),
        D((S,)), D((S,)), D((S,)), D((S,)), D((S,)), D((S,)), D((T,)), D((T,)), D, D,
        D((R,)), D((R,)), D((T,)), D((T,)), D((4,)), D((4,)), D((2,)), D((2,)),
    ]
    return pl.pallas_call(
        functools.partial(mixer_kernel, S, T),
        out_shape=jax.ShapeDtypeStruct((n, da), BF),
        in_specs=[pl.BlockSpec(memory_space=pltpu.VMEM)] * len(args),
        out_specs=pl.BlockSpec(memory_space=pltpu.VMEM),
        scratch_shapes=scratch,
        compiler_params=pltpu.CompilerParams(
            collective_id=0, has_side_effects=True, vmem_limit_bytes=60 * 1024 * 1024
        ),
    )(*args)


def solution(mesh):
    placed = (
        P("sp", "tp"),
        P("tp"),
        P("sp", "tp"),
        P("sp", "tp"),
        P("sp", "tp"),
        P("sp", "tp"),
        P("sp", "tp"),
        P("sp", "tp"),
        P("tp", None, None),
        P("tp"),
        P(None, "tp"),
        P(None, "tp"),
        P(None, "tp"),
        P("tp"),
        P("tp"),
        P("sp", "tp"),
        P("tp"),
        P("tp"),
        P("tp", "sp"),
        P("tp", "sp"),
    )
    S, T = mesh.shape["sp"], mesh.shape["tp"]

    def chosen(*args):
        if fits(S, T, [a.shape for a in args]):
            return fused(S, T, *args)
        return local(*args)

    return jax.shard_map(
        chosen, mesh=mesh, in_specs=placed, out_specs=P("sp", "tp"), check_vma=False
    )
```

```python
import functools

import jax
import jax.numpy as jnp
from jax import lax
from jax.experimental import pallas as pl
from jax.experimental.pallas import tpu as pltpu
from jax.sharding import PartitionSpec as P

SSM_STATE = 64
POOL_GROUPS = 4
SCAN_BLOCK = 128
MIX_W = 1024


EPSILON = 1e-06
HIGH = lax.Precision.HIGHEST


def shifted(value, axis, steps):
    count = lax.axis_size(axis)
    leading, last = (max(0, -steps), min(count, count - steps))
    return lax.ppermute(value, axis, [(source, source + steps) for source in range(leading, last)])


def carried_in(part, axis, combine, identity):
    place = lax.axis_index(axis)
    gathered = jax.tree.map(lambda a: lax.all_gather(a, axis), part)
    state = jax.tree.map(lambda a, e: jnp.zeros_like(a) + jnp.asarray(e, a.dtype), part, identity)

    def one(step, state):
        return combine(
            state, jax.tree.map(lambda a: lax.dynamic_index_in_dim(a, step, 0, False), gathered)
        )

    return lax.fori_loop(0, place, one, state)


def backward_kernel(extended, taps):
    width = taps.shape[0]
    length = extended.shape[0] - (width - 1)
    widened_rows = extended.astype(jnp.float32)
    total = jnp.zeros((length, extended.shape[1]), jnp.float32)
    for offset in range(width):
        total = total + taps[offset][None, :] * widened_rows[offset : offset + length]
    return jax.nn.silu(total).astype(jnp.bfloat16)


def combine_states(preceding_token, later):
    return (preceding_token[0] * later[0], preceding_token[1] * later[0][:, None, None] + later[1])


def local(
    activations,
    norm_gain,
    pool_weight,
    gate_weight,
    value_weight,
    key_weight,
    read_weight,
    step_weight,
    pool_mix,
    pool_scale,
    taps_value,
    taps_key,
    taps_read,
    step_bias,
    decay_log,
    decay_extra,
    skip_scale,
    state_gain,
    out_pool_weight,
    out_state_weight,
):
    length = activations.shape[0]
    cluster_span = pool_weight.shape[1]
    local_mix = gate_weight.shape[1]
    local_state = key_weight.shape[1]
    local_heads = step_weight.shape[1]
    joined = jnp.concatenate(
        [pool_weight, gate_weight, value_weight, key_weight, read_weight, step_weight], axis=1
    )
    in_weight = lax.all_gather(joined, "sp", axis=0, tiled=True)
    whole, gains = (
        lax.all_gather(activations, "tp", axis=1, tiled=True),
        lax.all_gather(norm_gain, "tp", axis=0, tiled=True),
    )
    widened_rows = whole.astype(jnp.float32)
    normed = (
        widened_rows
        * lax.rsqrt(jnp.mean(widened_rows * widened_rows, axis=-1, keepdims=True) + EPSILON)
        * gains.astype(jnp.float32)
    ).astype(jnp.bfloat16)
    projected = jnp.dot(normed, in_weight, preferred_element_type=jnp.float32)
    column = 0
    pool_in = projected[:, column : column + cluster_span].astype(jnp.bfloat16)
    column = column + cluster_span
    gate_in = projected[:, column : column + local_mix].astype(jnp.bfloat16)
    column = column + local_mix
    raw_value = projected[:, column : column + local_mix].astype(jnp.bfloat16)
    column = column + local_mix
    raw_key = projected[:, column : column + local_state].astype(jnp.bfloat16)
    column = column + local_state
    raw_read = projected[:, column : column + local_state].astype(jnp.bfloat16)
    column = column + local_state
    step_raw = projected[:, column : column + local_heads]
    raw_joined = jnp.concatenate([raw_value, raw_key, raw_read], axis=1)
    reach = 2**POOL_GROUPS - 1
    width = taps_value.shape[0]
    prior_pool, prior_joined = shifted(
        (pool_in[length - reach :], raw_joined[length - width + 1 :]), "sp", 1
    )
    group = lax.axis_index("tp")
    running = jnp.concatenate([prior_pool, pool_in], axis=0).astype(jnp.float32)
    levels = []
    for level in range(POOL_GROUPS):
        stride = 2**level
        running = running[stride:] + running[:-stride]
        levels.append(running[running.shape[0] - length :])
    window_sum = lax.dynamic_index_in_dim(jnp.stack(levels), group, 0, keepdims=False)
    window = jnp.exp2((group + 1).astype(jnp.float32))
    position = (lax.axis_index("sp") * length + jnp.arange(length, dtype=jnp.int32)).astype(
        jnp.float32
    )
    counts = jnp.minimum(position + 1.0, window)
    pooled = (window_sum / counts[:, None] - pool_in.astype(jnp.float32)).astype(jnp.bfloat16)
    pool_out = (
        jnp.dot(pooled, pool_mix[0], preferred_element_type=jnp.float32) * pool_scale
    ).astype(jnp.bfloat16)
    all_taps = jnp.concatenate([taps_value, taps_key, taps_read], axis=1)
    convolved = backward_kernel(jnp.concatenate([prior_joined, raw_joined], axis=0), all_taps)
    head_value = convolved[:, :local_mix]
    key_vectors = convolved[:, local_mix : local_mix + local_state]
    read_vectors = convolved[:, local_mix + local_state :]
    head_dim = local_mix // local_heads
    groups_here = local_state // SSM_STATE
    repeat = local_heads // groups_here
    blocks = length // SCAN_BLOCK
    step_size = jax.nn.softplus(step_raw + step_bias)
    log_decay = -jnp.exp(decay_log) * step_size + decay_extra
    value_heads = head_value.astype(jnp.float32).reshape(length, local_heads, head_dim)
    value_blocks = value_heads.reshape(blocks, SCAN_BLOCK, local_heads, head_dim)
    key_blocks = jnp.repeat(
        key_vectors.astype(jnp.float32).reshape(length, groups_here, SSM_STATE), repeat, axis=1
    ).reshape(blocks, SCAN_BLOCK, local_heads, SSM_STATE)
    read_blocks = jnp.repeat(
        read_vectors.astype(jnp.float32).reshape(length, groups_here, SSM_STATE), repeat, axis=1
    ).reshape(blocks, SCAN_BLOCK, local_heads, SSM_STATE)
    step_blocks = step_size.reshape(blocks, SCAN_BLOCK, local_heads)
    running_decay = jnp.cumsum(log_decay.reshape(blocks, SCAN_BLOCK, local_heads), axis=1)
    lower = jnp.arange(SCAN_BLOCK)[:, None] >= jnp.arange(SCAN_BLOCK)[None, :]
    gaps = jnp.where(
        lower[None, :, :, None],
        running_decay[:, :, None, :] - running_decay[:, None, :, :],
        -jnp.inf,
    )
    weights = jnp.einsum("blhn,bshn->blsh", read_blocks, key_blocks, precision=HIGH) * jnp.exp(gaps)
    scaled_value = value_blocks * step_blocks[..., None]
    inner = jnp.einsum("blsh,bshp->blhp", weights, scaled_value, precision=HIGH)
    block_ends = running_decay[:, -1, :]
    trailing = jnp.exp(block_ends[:, None, :] - running_decay)
    fresh = jnp.einsum("bshn,bsh,bshp->bhpn", key_blocks, trailing, scaled_value, precision=HIGH)

    def advance(carry, inputs):
        block_decay, block_state = inputs
        return (carry * block_decay[:, None, None] + block_state, carry)

    local_total, prefix = lax.scan(
        advance,
        jnp.zeros((local_heads, head_dim, SSM_STATE), jnp.float32),
        (jnp.exp(block_ends), fresh),
    )
    offsets = jnp.cumsum(block_ends, axis=0) - block_ends
    device_decay = jnp.exp(offsets[-1] + block_ends[-1])
    incoming_decay, incoming = carried_in(
        (device_decay, local_total),
        "sp",
        combine_states,
        (jnp.ones_like(device_decay), jnp.zeros_like(local_total)),
    )
    from_device = running_decay + offsets[:, None, :]
    local_off = (
        jnp.einsum("blhn,bhpn->blhp", read_blocks, prefix, precision=HIGH)
        * jnp.exp(running_decay)[..., None]
    )
    far_off = (
        jnp.einsum("blhn,hpn->blhp", read_blocks, incoming, precision=HIGH)
        * jnp.exp(from_device)[..., None]
    )
    scan_out = (inner + local_off + far_off).reshape(length, local_heads, head_dim) + skip_scale[
        None, :, None
    ] * value_heads
    gated = scan_out.reshape(length, local_mix) * jax.nn.silu(gate_in.astype(jnp.float32))
    gate_squares = lax.psum(jnp.sum(gated * gated, axis=-1), "tp")
    state_out = (gated * lax.rsqrt(gate_squares / MIX_W + EPSILON)[:, None] * state_gain).astype(
        jnp.bfloat16
    )
    branch_rows = jnp.concatenate([pool_out, state_out], axis=1)
    out_weight = jnp.concatenate([out_pool_weight, out_state_weight], axis=0)
    terms = jnp.dot(
        branch_rows,
        lax.all_gather(out_weight, "sp", axis=1, tiled=True),
        preferred_element_type=jnp.float32,
    )
    result = lax.psum_scatter(terms, "tp", scatter_dimension=1, tiled=True)
    return result.astype(jnp.bfloat16)


BF = jnp.bfloat16
F32 = jnp.float32
MESH = pl.DeviceIdType.MESH


def flip(index, mask):
    bit = 1
    while bit <= mask:
        if mask & bit:
            index = index + bit - 2 * bit * lax.rem(lax.div(index, bit), 2)
        bit *= 2
    return index


class Stream:
    def __init__(self, axis, place, bits, refs, send_sems, recv_sems, base, started):
        self.axis, self.place, self.bits, self.refs = axis, place, bits, refs
        self.send_sems, self.recv_sems, self.base, self.started = send_sems, recv_sems, base, started

    def via(self, mask):
        return [bit for bit in self.bits if mask & bit][-1]

    def copy(self, mask, bit):
        ref = self.refs(flip(self.place, mask))
        slot = self.base + (mask | bit)
        return pltpu.make_async_remote_copy(
            src_ref=ref, dst_ref=ref, send_sem=self.send_sems.at[slot], recv_sem=self.recv_sems.at[slot],
            device_id={self.axis: flip(self.place, bit)}, device_id_type=MESH,
        )

    def push(self, mask):
        onward = self.bits if mask == 0 else self.bits[self.bits.index(self.via(mask)) + 1 :]
        for bit in sorted(onward):
            c = self.copy(mask, bit)
            c.start()
            self.started.append(c)

    def got(self, mask):
        ref = self.refs(flip(self.place, mask))
        slot = self.base + mask
        pltpu.make_async_remote_copy(
            src_ref=ref, dst_ref=ref, send_sem=self.send_sems.at[slot], recv_sem=self.recv_sems.at[slot],
            device_id={self.axis: flip(self.place, self.via(mask))}, device_id_type=MESH,
        ).wait_recv()
        self.push(mask)


def early_first(size):
    return [m for m in range(2, size) if m // 2 & (m // 2 - 1) == 0 and m > 3]


def bt(a, b, **kw):
    return lax.dot_general(a, b, (((1,), (1,)), ((), ())), preferred_element_type=F32, **kw)


def halves(x):
    top = x.astype(BF)
    return top, (x - top.astype(F32)).astype(BF)


def mixer_kernel(
    S, T,
    act, gain, pool_w, gate_w, value_w, key_w, read_w, step_t, mix, scale, taps_v, taps_k, taps_r,
    bias, dlog, extra_t, skip, sgain, opool, ostate,
    out,
    wbuf, sbuf, obuf, abuf, nbuf, acc, sacc, ext, conv, hsend, hrecv, scan, xs, xr, ssend, srecv,
    brow, psend, precv, pown, qsend, qrecv, expd,
    w_ss, w_rs, s_ss, s_rs, o_ss, o_rs, a_ss, a_rs, h_ss, h_rs, x_ss, x_rs, q_ss, q_rs, p_ss, p_rs, r_ss, r_rs,
):
    n, da = act.shape
    kd = pool_w.shape[0]
    cw = pool_w.shape[1]
    st = key_w.shape[0]
    ncol = wbuf.shape[2]
    blk = SCAN_BLOCK
    blocks = n // blk
    hd = SSM_STATE
    me = lax.axis_index("sp")
    tp = lax.axis_index("tp")
    wbuf[me, :, 0:cw] = pool_w[...]
    wbuf[me, :, cw : 2 * cw] = gate_w[...]
    wbuf[me, :, 2 * cw : 3 * cw] = value_w[...]
    eye_kd = jnp.where(
        lax.broadcasted_iota(jnp.int32, (kd, kd), 0) == lax.broadcasted_iota(jnp.int32, (kd, kd), 1), 1.0, 0.0
    ).astype(BF)
    wbuf[me, :, 3 * cw :] = bt(eye_kd, jnp.concatenate([key_w[...], read_w[...]], axis=0)).astype(BF)
    hp = sbuf.shape[1]
    heads = step_t.shape[0]
    pick = jnp.where(
        lax.broadcasted_iota(jnp.int32, (hp, heads), 0) == lax.broadcasted_iota(jnp.int32, (hp, heads), 1), 1.0, 0.0
    ).astype(F32)
    sbuf[me] = jnp.dot(pick.astype(BF), step_t[...], preferred_element_type=F32).astype(BF)
    abuf[tp, 0:n, :] = act[...]
    abuf[tp, n : n + 16, :] = jnp.broadcast_to(gain[...].astype(F32), (16, da)).astype(BF)

    barrier = pltpu.get_barrier_semaphore()
    for k in range(1, S):
        pl.semaphore_signal(barrier, inc=1, device_id={"sp": lax.rem(me + k, S)}, device_id_type=MESH)
    for k in range(1, T):
        pl.semaphore_signal(barrier, inc=1, device_id={"tp": lax.rem(tp + k, T)}, device_id_type=MESH)
    obuf[me, 0:cw, :] = opool[...]
    obuf[me, cw:, :] = ostate[...]
    pl.semaphore_wait(barrier, S - 1 + T - 1)

    started = []

    def remote(src, dst, ss, rs, **peer):
        c = pltpu.make_async_remote_copy(
            src_ref=src, dst_ref=dst, send_sem=ss, recv_sem=rs, device_id=peer, device_id_type=MESH
        )
        return c

    def send(*a, **k):
        c = remote(*a, **k)
        c.start()
        started.append(c)

    far = [1 << k for k in reversed(range(1, S.bit_length() - 1))]
    late = far + [1]
    early = [1] + far
    cut = -(-kd // 96) * 16
    ocut = cut * 2 * cw // kd
    wq = Stream("sp", me, late, lambda i: wbuf.at[i, pl.ds(cut, kd - cut)], w_ss, w_rs, 0, started)
    wp = Stream("sp", me, early, lambda i: wbuf.at[i, pl.ds(0, cut)], w_ss, w_rs, S, started)
    sq_ = Stream("sp", me, late, lambda i: sbuf.at[i], s_ss, s_rs, 0, started)
    oq = Stream("sp", me, late, lambda i: obuf.at[i, pl.ds(ocut, 2 * cw - ocut)], o_ss, o_rs, 0, started)
    op = Stream("sp", me, early, lambda i: obuf.at[i, pl.ds(0, ocut)], o_ss, o_rs, S, started)
    aa = Stream("tp", tp, [1 << k for k in reversed(range(T.bit_length() - 1))], lambda i: abuf.at[i], a_ss, a_rs, 0, started)
    masks = sorted(range(1, S), key=lambda m: (bin(m).count("1"), m))
    even = [m for m in masks if m % 2 == 0]
    odd = [m for m in masks if m % 2 == 1]
    wp.push(0)
    wq.push(0)
    sq_.push(0)
    aa.push(0)
    wp.got(1)
    aa.got(2)
    wq.got(even[0])
    sq_.got(even[0])
    for mask in range(1, T):
        if mask != 2:
            aa.got(mask)
    per = da // kd
    rt = 64

    def norm_rows(i, _):
        r = pl.ds(pl.multiple_of(i * rt, rt), rt)
        parts = [abuf[t, r, :].astype(F32) for t in range(T)]
        tot = sum(jnp.sum(p * p, axis=-1, keepdims=True) for p in parts)
        rs = lax.rsqrt(tot / (da * T) + EPSILON)
        for t in range(T):
            g = abuf[t, n : n + 1, :].astype(F32)
            v = (parts[t] * rs * g).astype(BF)
            for j in range(per):
                nbuf[t * per + j, r, :] = v[:, j * kd : (j + 1) * kd]
        return 0

    lax.fori_loop(0, n // rt, norm_rows, 0)
    mt = 256

    def add_chunk(i, first):
        for r0 in range(0, n, mt):
            x = nbuf[i, r0 : r0 + mt, :]
            d = jnp.dot(x, wbuf[i], preferred_element_type=F32)
            if first:
                acc[r0 : r0 + mt, :] = d
            else:
                acc[r0 : r0 + mt, :] += d
        d = bt(sbuf[i], nbuf[i])
        if first:
            sacc[...] = d
        else:
            sacc[...] += d

    add_chunk(me, True)
    for k, mask in enumerate(even):
        if k:
            wq.got(mask)
            sq_.got(mask)
        if k == 1:
            for m in early_first(S):
                wp.got(m)
        if k == len(even) - 1:
            op.push(0)
            oq.push(0)
    rest = [m for m in masks if m != 1 and m not in early_first(S)]
    for mask in even:
        if mask in rest:
            wp.got(mask)
        add_chunk(flip(me, mask), False)
    for mask in odd:
        if mask in rest:
            wp.got(mask)
        wq.got(mask)
        sq_.got(mask)
        add_chunk(flip(me, mask), False)

    raw0 = 16
    ccol = ncol - cw
    hsend[:, 0:cw] = acc[n - raw0 :, 0:cw].astype(BF)
    hsend[:, cw:] = acc[n - raw0 :, 2 * cw :].astype(BF)

    def halo():
        return remote(hsend, hrecv, h_ss, h_rs, sp=lax.rem(me + 1, S))

    @pl.when(me < S - 1)
    def _():
        halo().start()

    ext[raw0:, 0:cw] = acc[:, 0:cw].astype(BF).astype(F32)
    ext[raw0:, cw:] = acc[:, 2 * cw :].astype(BF).astype(F32)

    def column(row):
        return bt(pick, jnp.broadcast_to(row[...], (8, heads)), precision=HIGH)[:, 0:1]

    step = sacc[...] + column(bias)
    step = jnp.maximum(step, 0.0) + jnp.log1p(jnp.exp(-jnp.abs(step)))
    ld = -jnp.exp(column(dlog)) * step + jnp.dot(pick, extra_t[...], precision=HIGH, preferred_element_type=F32)
    r_i = lax.broadcasted_iota(jnp.int32, (blk, blk), 0)
    c_i = lax.broadcasted_iota(jnp.int32, (blk, blk), 1)
    upper = jnp.where(r_i <= c_i, 1.0, 0.0).astype(F32)
    eye = jnp.where(r_i == c_i, 1.0, 0.0).astype(F32)
    lower = r_i >= c_i
    expand = jnp.where(
        lax.broadcasted_iota(jnp.int32, (hp, cw), 1) // hd == lax.broadcasted_iota(jnp.int32, (hp, cw), 0), 1.0, 0.0
    ).astype(F32)
    skips = jnp.dot(
        jnp.broadcast_to(skip[...], (8, heads)), expand[0:heads, :], precision=HIGH, preferred_element_type=F32
    )[0:1, :]
    eye_st = jnp.where(
        lax.broadcasted_iota(jnp.int32, (st, st), 0) == lax.broadcasted_iota(jnp.int32, (st, st), 1), 1.0, 0.0
    ).astype(BF)
    cum_rs, cum_cs, st_rs, wexps = [], [], [], []
    for b in range(blocks):
        cols = slice(b * blk, (b + 1) * blk)
        cum_r = jnp.dot(ld[:, cols], upper, precision=HIGH, preferred_element_type=F32)
        st_r = step[:, cols]
        turned = bt(eye, jnp.concatenate([cum_r, st_r], axis=0), precision=HIGH)
        cum_c = turned[:, 0:hp]
        w_c = jnp.exp(cum_c[blk - 1 : blk, :] - cum_c) * turned[:, hp:]
        both = jnp.dot(
            jnp.concatenate([w_c, jnp.exp(cum_c)], axis=0), expand, precision=HIGH, preferred_element_type=F32
        )
        expd[cols, :] = both[blk:, :]
        wexps.append(both[:blk, :])
        cum_rs.append(cum_r)
        cum_cs.append(cum_c)
        st_rs.append(st_r)

    @pl.when(me > 0)
    def _():
        halo().wait_recv()
        ext[0:raw0, :] = hrecv[...].astype(F32)

    @pl.when(me == 0)
    def _():
        ext[0:raw0, :] = jnp.zeros((raw0, ext.shape[1]), F32)

    width = taps_v.shape[0]
    for b in range(blocks):
        for taps, lo, hi in ((taps_v, 0, cw), (taps_k, cw, cw + st), (taps_r, cw + st, cw + 2 * st)):
            total = jnp.zeros((blk, hi - lo), F32)
            for k in range(width):
                o = b * blk + raw0 - (width - 1) + k
                total = total + taps[k : k + 1, :] * ext[o : o + blk, cw + lo : cw + hi]
            conv[b * blk : (b + 1) * blk, lo:hi] = (total * jax.nn.sigmoid(total)).astype(BF)

    run = jnp.zeros((st, cw), F32)
    dec = jnp.ones((1, cw), F32)
    pres, offs = [], []
    for b in range(blocks):
        rows = slice(b * blk, (b + 1) * blk)
        key_t = bt(eye_st, conv[rows, cw : cw + st]).astype(BF)
        sv = conv[rows, 0:cw].astype(F32) * wexps[b]
        top, low = halves(sv)
        new = jnp.dot(key_t, top, preferred_element_type=F32) + jnp.dot(key_t, low, preferred_element_type=F32)
        bd = expd[(b + 1) * blk - 1 : (b + 1) * blk, :]
        pres.append(run)
        offs.append(dec)
        run = run * bd + new
        dec = dec * bd

    in_s = jnp.zeros((st, cw), F32)
    in_d = jnp.ones((1, cw), F32)
    rounds = [1 << k for k in range(S.bit_length() - 1)]

    def inner(b):
        rows = slice(b * blk, (b + 1) * blk)
        g = bt(conv[rows, cw + st :], conv[rows, cw : cw + st])
        for h in range(cw // hd):
            gap = jnp.where(lower, cum_cs[b][:, h : h + 1] - cum_rs[b][h : h + 1, :], -jnp.inf)
            wm = g * jnp.exp(gap) * st_rs[b][h : h + 1, :]
            top, low = halves(wm)
            v = conv[rows, h * hd : (h + 1) * hd]
            scan[rows, h * hd : (h + 1) * hd] = jnp.dot(top, v, preferred_element_type=F32) + jnp.dot(
                low, v, preferred_element_type=F32
            )

    window = lax.shift_left(jnp.int32(2), tp)
    back = (
        lax.broadcasted_iota(jnp.int32, (blk, blk + raw0), 0)
        + raw0
        - lax.broadcasted_iota(jnp.int32, (blk, blk + raw0), 1)
    )
    band = jnp.where((back >= 0) & (back < window), 1.0, 0.0).astype(BF)

    def pool(b):
        rows = slice(b * blk, (b + 1) * blk)
        sums = jnp.dot(band, ext[b * blk : (b + 1) * blk + raw0, 0:cw].astype(BF), preferred_element_type=F32)
        pos = (me * n + b * blk + lax.broadcasted_iota(jnp.int32, (blk, cw), 0)).astype(F32)
        counts = jnp.minimum(pos + 1.0, window.astype(F32))
        pooled = (sums / counts - ext[b * blk + raw0 : (b + 1) * blk + raw0, 0:cw]).astype(BF)
        brow[rows, 0:cw] = (jnp.dot(pooled, mix[0], preferred_element_type=F32) * scale[...]).astype(BF)

    work = [functools.partial(inner, b) for b in range(blocks)] + [functools.partial(pool, b) for b in range(blocks)]
    share = -(-len(work) // len(rounds))
    o_left = [(op, 1), (oq, even[0])] + [(op, m) for m in early_first(S)] + [(oq, m) for m in even[1:]]
    o_step = -(-len(o_left) // len(rounds))
    o_rest = [(op, m) for m in masks if (op, m) not in o_left] + [(oq, m) for m in odd]

    def take_o(count):
        for stream, mask in o_left[:count]:
            stream.got(mask)
        del o_left[:count]

    for r, bit in enumerate(rounds):
        xs[r, 0:st, :] = run
        xs[r, st:, :] = jnp.broadcast_to(dec, (xs.shape[1] - st, cw))
        send(xs.at[r], xr.at[r], x_ss.at[r], x_rs.at[r], sp=flip(me, bit))
        for f in work[r * share : (r + 1) * share]:
            f()
        take_o(o_step)
        remote(xs.at[r], xr.at[r], x_ss.at[r], x_rs.at[r], sp=flip(me, bit)).wait_recv()
        other, odec = xr[r, 0:st, :], xr[r, st : st + 1, :]
        later = lax.rem(lax.div(me, bit), 2) == 1
        in_s = jnp.where(later, other * in_d + in_s, in_s)
        in_d = jnp.where(later, odec * in_d, in_d)
        run = jnp.where(later, other * dec + run, run * odec + other)
        dec = dec * odec

    for b in range(blocks):
        rows = slice(b * blk, (b + 1) * blk)
        top, low = halves(pres[b] + offs[b] * in_s)
        rd = conv[rows, cw + st :]
        carried = jnp.dot(rd, top, preferred_element_type=F32) + jnp.dot(rd, low, preferred_element_type=F32)
        y = scan[rows, :] + carried * expd[rows, :] + skips * conv[rows, 0:cw].astype(F32)
        gt = acc[rows, cw : 2 * cw].astype(BF).astype(F32)
        gated = y * (gt * jax.nn.sigmoid(gt))
        ssend[:, rows] = bt(jnp.ones((8, cw), F32), gated * gated, precision=HIGH)
        brow[rows, cw:] = (gated * sgain[...]).astype(BF)
    for k in range(1, T):
        send(ssend, srecv.at[k - 1], q_ss.at[k - 1], q_rs.at[k - 1], tp=flip(tp, k))
    take_o(len(o_left))
    for stream, mask in o_rest:
        stream.got(mask)
    for k in range(1, T):
        remote(ssend, srecv.at[k - 1], q_ss.at[k - 1], q_rs.at[k - 1], tp=flip(tp, k)).wait_recv()
    sq = ssend[...]
    for k in range(1, T):
        sq = sq + srecv[k - 1]
    rs_row = lax.rsqrt(sq / (cw * T) + EPSILON)
    rs_cols = [bt(eye, rs_row[:, b * blk : (b + 1) * blk], precision=HIGH)[:, 0:1] for b in range(blocks)]
    wide = S // T
    oc = obuf.shape[2]
    parts = 4
    pr = n // parts

    def product(t, part, store):
        rows = slice(part * pr, (part + 1) * pr)
        rs = jnp.concatenate(rs_cols[part * blocks // parts : (part + 1) * blocks // parts], axis=0)
        for j in range(wide):
            i = t * wide + j
            p = jnp.dot(brow[rows, 0:cw], obuf[i, 0:cw, :], preferred_element_type=F32)
            p = p + rs * jnp.dot(brow[rows, cw:], obuf[i, cw:, :], preferred_element_type=F32)
            store(rows, slice(j * oc, (j + 1) * oc), p)

    def into(ref, *lead):
        def store(rows, cols, p):
            ref[lead + (rows, cols)] = p.astype(ref.dtype)
        return store

    near = flip(tp, 1)

    def near_copy(k, part):
        rows = pl.ds(part * pr, pr)
        i = k * parts + part
        return remote(psend.at[k, rows], precv.at[k, rows], p_ss.at[i], p_rs.at[i], tp=near)

    def far_copy(part):
        rows = pl.ds(part * pr, pr)
        return remote(qsend.at[rows], qrecv.at[rows], r_ss.at[part], r_rs.at[part], tp=flip(tp, 2))

    for part in range(parts):
        product(flip(tp, 3), part, into(psend, 0))
        near_copy(0, part).start()
    for part in range(parts):
        rows = slice(part * pr, (part + 1) * pr)
        product(flip(tp, 2), part, into(pown))
        near_copy(0, part).wait_recv()
        qsend[rows, :] = (pown[rows, :] + precv[0, rows, :]).astype(BF)
        far_copy(part).start()
    for part in range(parts):
        product(near, part, into(psend, 1))
        near_copy(1, part).start()
    for part in range(parts):
        product(tp, part, into(pown))
    for part in range(parts):
        rows = slice(part * pr, (part + 1) * pr)
        near_copy(1, part).wait_recv()
        far_copy(part).wait_recv()
        out[rows, :] = (pown[rows, :] + precv[1, rows, :] + qrecv[rows, :].astype(F32)).astype(out.dtype)

    for c in started:
        c.wait_send()
    for part in range(parts):
        near_copy(0, part).wait_send()
        near_copy(1, part).wait_send()
        far_copy(part).wait_send()

    @pl.when(me < S - 1)
    def _():
        halo().wait_send()


def fits(S, T, shapes):
    n, da = shapes[0]
    kd, cw = shapes[2]
    st = shapes[5][1]
    oc = shapes[18][1]
    heads = shapes[7][1]
    return (
        T == 4 == POOL_GROUPS and S >= T and S & (S - 1) == 0 and S <= 16 and st == SSM_STATE
        and cw == heads * SSM_STATE and n % (4 * SCAN_BLOCK) == 0
        and -(-kd // 96) * 2 * cw % kd == 0 and oc % 128 == 0 and kd % 128 == 0 and da % kd == 0
        and n % (2 * SCAN_BLOCK) == 0 and cw % 128 == 0 and oc * S == da * T
    )


def fused(
    S, T, activations, norm_gain, pool_weight, gate_weight, value_weight, key_weight, read_weight,
    step_weight, pool_mix, pool_scale, taps_value, taps_key, taps_read, step_bias, decay_log,
    decay_extra, skip_scale, state_gain, out_pool_weight, out_state_weight,
):
    n, da = activations.shape
    kd, cw = pool_weight.shape
    st = key_weight.shape[1]
    heads = step_weight.shape[1]
    oc = out_pool_weight.shape[1]
    hp = 16
    args = (
        activations, norm_gain[None, :], pool_weight, gate_weight, value_weight, key_weight.T, read_weight.T,
        step_weight.T, pool_mix, pool_scale[None, :], taps_value, taps_key, taps_read, step_bias[None, :], decay_log[None, :],
        decay_extra.T, skip_scale[None, :], state_gain[None, :],
        out_pool_weight, out_state_weight,
    )
    ncol = 3 * cw + 2 * st
    ccol = ncol - cw
    V = pltpu.VMEM
    D = pltpu.SemaphoreType.DMA
    R = S.bit_length() - 1
    scratch = [
        V((S, kd, ncol), BF), V((S, hp, kd), BF), V((S, 2 * cw, oc), BF), V((T, n + 16, da), BF),
        V((S, n, kd), BF), V((n, ncol), F32), V((hp, n), F32), V((n + 16, ccol), F32),
        V((n, cw + 2 * st), BF), V((16, ccol), BF), V((16, ccol), BF), V((n, cw), F32),
        V((R, st + 8, cw), F32), V((R, st + 8, cw), F32), V((8, n), F32), V((T - 1, 8, n), F32),
        V((n, 2 * cw), BF), V((2, n, da), F32), V((2, n, da), F32), V((n, da), F32),
        V((n, da), BF), V((n, da), BF), V((n, cw), F32),
        D((2 * S,)), D((2 * S,)), D((S,)), D((S,)), D((2 * S,)), D((2 * S,)), D((T,)), D((T,)), D, D,
        D((R,)), D((R,)), D((T,)), D((T,)), D((8,)), D((8,)), D((4,)), D((4,)),
    ]
    return pl.pallas_call(
        functools.partial(mixer_kernel, S, T),
        out_shape=jax.ShapeDtypeStruct((n, da), BF),
        in_specs=[pl.BlockSpec(memory_space=pltpu.VMEM)] * len(args),
        out_specs=pl.BlockSpec(memory_space=pltpu.VMEM),
        scratch_shapes=scratch,
        compiler_params=pltpu.CompilerParams(
            collective_id=0, has_side_effects=True, vmem_limit_bytes=60 * 1024 * 1024
        ),
    )(*args)


def solution(mesh):
    placed = (
        P("sp", "tp"),
        P("tp"),
        P("sp", "tp"),
        P("sp", "tp"),
        P("sp", "tp"),
        P("sp", "tp"),
        P("sp", "tp"),
        P("sp", "tp"),
        P("tp", None, None),
        P("tp"),
        P(None, "tp"),
        P(None, "tp"),
        P(None, "tp"),
        P("tp"),
        P("tp"),
        P("sp", "tp"),
        P("tp"),
        P("tp"),
        P("tp", "sp"),
        P("tp", "sp"),
    )
    S, T = mesh.shape["sp"], mesh.shape["tp"]

    def chosen(*args):
        if fits(S, T, [a.shape for a in args]):
            return fused(S, T, *args)
        return local(*args)

    return jax.shard_map(
        chosen, mesh=mesh, in_specs=placed, out_specs=P("sp", "tp"), check_vma=False
    )
```

```python
import functools

import jax
import jax.numpy as jnp
from jax import lax
from jax.experimental import pallas as pl
from jax.experimental.pallas import tpu as pltpu
from jax.sharding import PartitionSpec as P

SSM_STATE = 64
POOL_GROUPS = 4
SCAN_BLOCK = 128
MIX_W = 1024


EPSILON = 1e-06
HIGH = lax.Precision.HIGHEST


def shifted(value, axis, steps):
    count = lax.axis_size(axis)
    leading, last = (max(0, -steps), min(count, count - steps))
    return lax.ppermute(value, axis, [(source, source + steps) for source in range(leading, last)])


def carried_in(part, axis, combine, identity):
    place = lax.axis_index(axis)
    gathered = jax.tree.map(lambda a: lax.all_gather(a, axis), part)
    state = jax.tree.map(lambda a, e: jnp.zeros_like(a) + jnp.asarray(e, a.dtype), part, identity)

    def one(step, state):
        return combine(
            state, jax.tree.map(lambda a: lax.dynamic_index_in_dim(a, step, 0, False), gathered)
        )

    return lax.fori_loop(0, place, one, state)


def backward_kernel(extended, taps):
    width = taps.shape[0]
    length = extended.shape[0] - (width - 1)
    widened_rows = extended.astype(jnp.float32)
    total = jnp.zeros((length, extended.shape[1]), jnp.float32)
    for offset in range(width):
        total = total + taps[offset][None, :] * widened_rows[offset : offset + length]
    return jax.nn.silu(total).astype(jnp.bfloat16)


def combine_states(preceding_token, later):
    return (preceding_token[0] * later[0], preceding_token[1] * later[0][:, None, None] + later[1])


def local(
    activations,
    norm_gain,
    pool_weight,
    gate_weight,
    value_weight,
    key_weight,
    read_weight,
    step_weight,
    pool_mix,
    pool_scale,
    taps_value,
    taps_key,
    taps_read,
    step_bias,
    decay_log,
    decay_extra,
    skip_scale,
    state_gain,
    out_pool_weight,
    out_state_weight,
):
    length = activations.shape[0]
    cluster_span = pool_weight.shape[1]
    local_mix = gate_weight.shape[1]
    local_state = key_weight.shape[1]
    local_heads = step_weight.shape[1]
    joined = jnp.concatenate(
        [pool_weight, gate_weight, value_weight, key_weight, read_weight, step_weight], axis=1
    )
    in_weight = lax.all_gather(joined, "sp", axis=0, tiled=True)
    whole, gains = (
        lax.all_gather(activations, "tp", axis=1, tiled=True),
        lax.all_gather(norm_gain, "tp", axis=0, tiled=True),
    )
    widened_rows = whole.astype(jnp.float32)
    normed = (
        widened_rows
        * lax.rsqrt(jnp.mean(widened_rows * widened_rows, axis=-1, keepdims=True) + EPSILON)
        * gains.astype(jnp.float32)
    ).astype(jnp.bfloat16)
    projected = jnp.dot(normed, in_weight, preferred_element_type=jnp.float32)
    column = 0
    pool_in = projected[:, column : column + cluster_span].astype(jnp.bfloat16)
    column = column + cluster_span
    gate_in = projected[:, column : column + local_mix].astype(jnp.bfloat16)
    column = column + local_mix
    raw_value = projected[:, column : column + local_mix].astype(jnp.bfloat16)
    column = column + local_mix
    raw_key = projected[:, column : column + local_state].astype(jnp.bfloat16)
    column = column + local_state
    raw_read = projected[:, column : column + local_state].astype(jnp.bfloat16)
    column = column + local_state
    step_raw = projected[:, column : column + local_heads]
    raw_joined = jnp.concatenate([raw_value, raw_key, raw_read], axis=1)
    reach = 2**POOL_GROUPS - 1
    width = taps_value.shape[0]
    prior_pool, prior_joined = shifted(
        (pool_in[length - reach :], raw_joined[length - width + 1 :]), "sp", 1
    )
    group = lax.axis_index("tp")
    running = jnp.concatenate([prior_pool, pool_in], axis=0).astype(jnp.float32)
    levels = []
    for level in range(POOL_GROUPS):
        stride = 2**level
        running = running[stride:] + running[:-stride]
        levels.append(running[running.shape[0] - length :])
    window_sum = lax.dynamic_index_in_dim(jnp.stack(levels), group, 0, keepdims=False)
    window = jnp.exp2((group + 1).astype(jnp.float32))
    position = (lax.axis_index("sp") * length + jnp.arange(length, dtype=jnp.int32)).astype(
        jnp.float32
    )
    counts = jnp.minimum(position + 1.0, window)
    pooled = (window_sum / counts[:, None] - pool_in.astype(jnp.float32)).astype(jnp.bfloat16)
    pool_out = (
        jnp.dot(pooled, pool_mix[0], preferred_element_type=jnp.float32) * pool_scale
    ).astype(jnp.bfloat16)
    all_taps = jnp.concatenate([taps_value, taps_key, taps_read], axis=1)
    convolved = backward_kernel(jnp.concatenate([prior_joined, raw_joined], axis=0), all_taps)
    head_value = convolved[:, :local_mix]
    key_vectors = convolved[:, local_mix : local_mix + local_state]
    read_vectors = convolved[:, local_mix + local_state :]
    head_dim = local_mix // local_heads
    groups_here = local_state // SSM_STATE
    repeat = local_heads // groups_here
    blocks = length // SCAN_BLOCK
    step_size = jax.nn.softplus(step_raw + step_bias)
    log_decay = -jnp.exp(decay_log) * step_size + decay_extra
    value_heads = head_value.astype(jnp.float32).reshape(length, local_heads, head_dim)
    value_blocks = value_heads.reshape(blocks, SCAN_BLOCK, local_heads, head_dim)
    key_blocks = jnp.repeat(
        key_vectors.astype(jnp.float32).reshape(length, groups_here, SSM_STATE), repeat, axis=1
    ).reshape(blocks, SCAN_BLOCK, local_heads, SSM_STATE)
    read_blocks = jnp.repeat(
        read_vectors.astype(jnp.float32).reshape(length, groups_here, SSM_STATE), repeat, axis=1
    ).reshape(blocks, SCAN_BLOCK, local_heads, SSM_STATE)
    step_blocks = step_size.reshape(blocks, SCAN_BLOCK, local_heads)
    running_decay = jnp.cumsum(log_decay.reshape(blocks, SCAN_BLOCK, local_heads), axis=1)
    lower = jnp.arange(SCAN_BLOCK)[:, None] >= jnp.arange(SCAN_BLOCK)[None, :]
    gaps = jnp.where(
        lower[None, :, :, None],
        running_decay[:, :, None, :] - running_decay[:, None, :, :],
        -jnp.inf,
    )
    weights = jnp.einsum("blhn,bshn->blsh", read_blocks, key_blocks, precision=HIGH) * jnp.exp(gaps)
    scaled_value = value_blocks * step_blocks[..., None]
    inner = jnp.einsum("blsh,bshp->blhp", weights, scaled_value, precision=HIGH)
    block_ends = running_decay[:, -1, :]
    trailing = jnp.exp(block_ends[:, None, :] - running_decay)
    fresh = jnp.einsum("bshn,bsh,bshp->bhpn", key_blocks, trailing, scaled_value, precision=HIGH)

    def advance(carry, inputs):
        block_decay, block_state = inputs
        return (carry * block_decay[:, None, None] + block_state, carry)

    local_total, prefix = lax.scan(
        advance,
        jnp.zeros((local_heads, head_dim, SSM_STATE), jnp.float32),
        (jnp.exp(block_ends), fresh),
    )
    offsets = jnp.cumsum(block_ends, axis=0) - block_ends
    device_decay = jnp.exp(offsets[-1] + block_ends[-1])
    incoming_decay, incoming = carried_in(
        (device_decay, local_total),
        "sp",
        combine_states,
        (jnp.ones_like(device_decay), jnp.zeros_like(local_total)),
    )
    from_device = running_decay + offsets[:, None, :]
    local_off = (
        jnp.einsum("blhn,bhpn->blhp", read_blocks, prefix, precision=HIGH)
        * jnp.exp(running_decay)[..., None]
    )
    far_off = (
        jnp.einsum("blhn,hpn->blhp", read_blocks, incoming, precision=HIGH)
        * jnp.exp(from_device)[..., None]
    )
    scan_out = (inner + local_off + far_off).reshape(length, local_heads, head_dim) + skip_scale[
        None, :, None
    ] * value_heads
    gated = scan_out.reshape(length, local_mix) * jax.nn.silu(gate_in.astype(jnp.float32))
    gate_squares = lax.psum(jnp.sum(gated * gated, axis=-1), "tp")
    state_out = (gated * lax.rsqrt(gate_squares / MIX_W + EPSILON)[:, None] * state_gain).astype(
        jnp.bfloat16
    )
    branch_rows = jnp.concatenate([pool_out, state_out], axis=1)
    out_weight = jnp.concatenate([out_pool_weight, out_state_weight], axis=0)
    terms = jnp.dot(
        branch_rows,
        lax.all_gather(out_weight, "sp", axis=1, tiled=True),
        preferred_element_type=jnp.float32,
    )
    result = lax.psum_scatter(terms, "tp", scatter_dimension=1, tiled=True)
    return result.astype(jnp.bfloat16)


BF = jnp.bfloat16
F32 = jnp.float32
MESH = pl.DeviceIdType.MESH


def flip(index, mask):
    bit = 1
    while bit <= mask:
        if mask & bit:
            index = index + bit - 2 * bit * lax.rem(lax.div(index, bit), 2)
        bit *= 2
    return index


class Stream:
    def __init__(self, axis, place, bits, refs, send_sems, recv_sems, base, started):
        self.axis, self.place, self.bits, self.refs = axis, place, bits, refs
        self.send_sems, self.recv_sems, self.base, self.started = send_sems, recv_sems, base, started

    def via(self, mask):
        return [bit for bit in self.bits if mask & bit][-1]

    def copy(self, mask, bit):
        ref = self.refs(flip(self.place, mask))
        slot = self.base + (mask | bit)
        return pltpu.make_async_remote_copy(
            src_ref=ref, dst_ref=ref, send_sem=self.send_sems.at[slot], recv_sem=self.recv_sems.at[slot],
            device_id={self.axis: flip(self.place, bit)}, device_id_type=MESH,
        )

    def push(self, mask):
        onward = self.bits if mask == 0 else self.bits[self.bits.index(self.via(mask)) + 1 :]
        for bit in sorted(onward):
            c = self.copy(mask, bit)
            c.start()
            self.started.append(c)

    def got(self, mask):
        ref = self.refs(flip(self.place, mask))
        slot = self.base + mask
        pltpu.make_async_remote_copy(
            src_ref=ref, dst_ref=ref, send_sem=self.send_sems.at[slot], recv_sem=self.recv_sems.at[slot],
            device_id={self.axis: flip(self.place, self.via(mask))}, device_id_type=MESH,
        ).wait_recv()
        self.push(mask)


def early_first(size):
    return [m for m in range(2, size) if m // 2 & (m // 2 - 1) == 0 and m > 3]


def bt(a, b, **kw):
    return lax.dot_general(a, b, (((1,), (1,)), ((), ())), preferred_element_type=F32, **kw)


def halves(x):
    top = x.astype(BF)
    return top, (x - top.astype(F32)).astype(BF)


def mixer_kernel(
    S, T,
    act, gain, pool_w, gate_w, value_w, key_w, read_w, step_t, mix, scale, taps_v, taps_k, taps_r,
    bias, dlog, extra_t, skip, sgain, opool, ostate,
    out,
    wbuf, sbuf, obuf, abuf, nbuf, acc, sacc, ext, conv, hsend, hrecv, scan, xs, xr, ssend, srecv,
    brow, psend, precv, pown, qsend, qrecv, expd,
    w_ss, w_rs, s_ss, s_rs, o_ss, o_rs, a_ss, a_rs, h_ss, h_rs, x_ss, x_rs, q_ss, q_rs, p_ss, p_rs, r_ss, r_rs,
):
    n, da = act.shape
    kd = pool_w.shape[0]
    cw = pool_w.shape[1]
    st = key_w.shape[0]
    ncol = wbuf.shape[2]
    blk = SCAN_BLOCK
    blocks = n // blk
    hd = SSM_STATE
    me = lax.axis_index("sp")
    tp = lax.axis_index("tp")
    wbuf[me, :, 0:cw] = pool_w[...]
    wbuf[me, :, cw : 2 * cw] = gate_w[...]
    wbuf[me, :, 2 * cw : 3 * cw] = value_w[...]
    eye_kd = jnp.where(
        lax.broadcasted_iota(jnp.int32, (kd, kd), 0) == lax.broadcasted_iota(jnp.int32, (kd, kd), 1), 1.0, 0.0
    ).astype(BF)
    wbuf[me, :, 3 * cw :] = bt(eye_kd, jnp.concatenate([key_w[...], read_w[...]], axis=0)).astype(BF)
    hp = sbuf.shape[1]
    heads = step_t.shape[0]
    pick = jnp.where(
        lax.broadcasted_iota(jnp.int32, (hp, heads), 0) == lax.broadcasted_iota(jnp.int32, (hp, heads), 1), 1.0, 0.0
    ).astype(F32)
    sbuf[me] = jnp.dot(pick.astype(BF), step_t[...], preferred_element_type=F32).astype(BF)
    abuf[tp, 0:n, :] = act[...]
    abuf[tp, n : n + 16, :] = jnp.broadcast_to(gain[...].astype(F32), (16, da)).astype(BF)

    barrier = pltpu.get_barrier_semaphore()
    for k in range(1, S):
        pl.semaphore_signal(barrier, inc=1, device_id={"sp": lax.rem(me + k, S)}, device_id_type=MESH)
    for k in range(1, T):
        pl.semaphore_signal(barrier, inc=1, device_id={"tp": lax.rem(tp + k, T)}, device_id_type=MESH)
    obuf[me, 0:cw, :] = opool[...]
    obuf[me, cw:, :] = ostate[...]
    pl.semaphore_wait(barrier, S - 1 + T - 1)

    started = []

    def remote(src, dst, ss, rs, **peer):
        c = pltpu.make_async_remote_copy(
            src_ref=src, dst_ref=dst, send_sem=ss, recv_sem=rs, device_id=peer, device_id_type=MESH
        )
        return c

    def send(*a, **k):
        c = remote(*a, **k)
        c.start()
        started.append(c)

    far = [1 << k for k in reversed(range(1, S.bit_length() - 1))]
    late = far + [1]
    early = [1] + far
    cut = -(-kd // 96) * 16
    ocut = cut * 2 * cw // kd
    wq = Stream("sp", me, late, lambda i: wbuf.at[i, pl.ds(cut, kd - cut)], w_ss, w_rs, 0, started)
    wp = Stream("sp", me, early, lambda i: wbuf.at[i, pl.ds(0, cut)], w_ss, w_rs, S, started)
    sq_ = Stream("sp", me, late, lambda i: sbuf.at[i], s_ss, s_rs, 0, started)
    oq = Stream("sp", me, late, lambda i: obuf.at[i, pl.ds(ocut, 2 * cw - ocut)], o_ss, o_rs, 0, started)
    op = Stream("sp", me, early, lambda i: obuf.at[i, pl.ds(0, ocut)], o_ss, o_rs, S, started)
    aa = Stream("tp", tp, [1 << k for k in reversed(range(T.bit_length() - 1))], lambda i: abuf.at[i], a_ss, a_rs, 0, started)
    masks = sorted(range(1, S), key=lambda m: (bin(m).count("1"), m))
    even = [m for m in masks if m % 2 == 0]
    odd = [m for m in masks if m % 2 == 1]
    wp.push(0)
    wq.push(0)
    sq_.push(0)
    aa.push(0)
    wp.got(1)
    aa.got(2)
    wq.got(even[0])
    sq_.got(even[0])
    for mask in range(1, T):
        if mask != 2:
            aa.got(mask)
    per = da // kd
    rt = 64

    def norm_rows(i, _):
        r = pl.ds(pl.multiple_of(i * rt, rt), rt)
        parts = [abuf[t, r, :].astype(F32) for t in range(T)]
        tot = sum(jnp.sum(p * p, axis=-1, keepdims=True) for p in parts)
        rs = lax.rsqrt(tot / (da * T) + EPSILON)
        for t in range(T):
            g = abuf[t, n : n + 1, :].astype(F32)
            v = (parts[t] * rs * g).astype(BF)
            for j in range(per):
                nbuf[t * per + j, r, :] = v[:, j * kd : (j + 1) * kd]
        return 0

    lax.fori_loop(0, n // rt, norm_rows, 0)
    mt = 256

    def add_chunk(i, first):
        for r0 in range(0, n, mt):
            x = nbuf[i, r0 : r0 + mt, :]
            d = jnp.dot(x, wbuf[i], preferred_element_type=F32)
            if first:
                acc[r0 : r0 + mt, :] = d
            else:
                acc[r0 : r0 + mt, :] += d
        d = bt(sbuf[i], nbuf[i])
        if first:
            sacc[...] = d
        else:
            sacc[...] += d

    add_chunk(me, True)
    for k, mask in enumerate(even):
        if k:
            wq.got(mask)
            sq_.got(mask)
        if k == 1:
            for m in early_first(S):
                wp.got(m)
        if k == min(1, len(even) - 1):
            op.push(0)
            oq.push(0)
    rest = [m for m in masks if m != 1 and m not in early_first(S)]
    for mask in even:
        if mask in rest:
            wp.got(mask)
        add_chunk(flip(me, mask), False)
    for mask in odd:
        if mask in rest:
            wp.got(mask)
        wq.got(mask)
        sq_.got(mask)
        add_chunk(flip(me, mask), False)

    raw0 = 16
    ccol = ncol - cw
    hsend[:, 0:cw] = acc[n - raw0 :, 0:cw].astype(BF)
    hsend[:, cw:] = acc[n - raw0 :, 2 * cw :].astype(BF)

    def halo():
        return remote(hsend, hrecv, h_ss, h_rs, sp=lax.rem(me + 1, S))

    @pl.when(me < S - 1)
    def _():
        halo().start()

    ext[raw0:, 0:cw] = acc[:, 0:cw].astype(BF).astype(F32)
    ext[raw0:, cw:] = acc[:, 2 * cw :].astype(BF).astype(F32)

    def column(row):
        return bt(pick, jnp.broadcast_to(row[...], (8, heads)), precision=HIGH)[:, 0:1]

    step = sacc[...] + column(bias)
    step = jnp.maximum(step, 0.0) + jnp.log1p(jnp.exp(-jnp.abs(step)))
    ld = -jnp.exp(column(dlog)) * step + jnp.dot(pick, extra_t[...], precision=HIGH, preferred_element_type=F32)
    r_i = lax.broadcasted_iota(jnp.int32, (blk, blk), 0)
    c_i = lax.broadcasted_iota(jnp.int32, (blk, blk), 1)
    upper = jnp.where(r_i <= c_i, 1.0, 0.0).astype(F32)
    eye = jnp.where(r_i == c_i, 1.0, 0.0).astype(F32)
    lower = r_i >= c_i
    expand = jnp.where(
        lax.broadcasted_iota(jnp.int32, (hp, cw), 1) // hd == lax.broadcasted_iota(jnp.int32, (hp, cw), 0), 1.0, 0.0
    ).astype(F32)
    skips = jnp.dot(
        jnp.broadcast_to(skip[...], (8, heads)), expand[0:heads, :], precision=HIGH, preferred_element_type=F32
    )[0:1, :]
    eye_st = jnp.where(
        lax.broadcasted_iota(jnp.int32, (st, st), 0) == lax.broadcasted_iota(jnp.int32, (st, st), 1), 1.0, 0.0
    ).astype(BF)
    cum_rs, cum_cs, st_rs, wexps = [], [], [], []
    for b in range(blocks):
        cols = slice(b * blk, (b + 1) * blk)
        cum_r = jnp.dot(ld[:, cols], upper, precision=HIGH, preferred_element_type=F32)
        st_r = step[:, cols]
        turned = bt(eye, jnp.concatenate([cum_r, st_r], axis=0), precision=HIGH)
        cum_c = turned[:, 0:hp]
        w_c = jnp.exp(cum_c[blk - 1 : blk, :] - cum_c) * turned[:, hp:]
        both = jnp.dot(
            jnp.concatenate([w_c, jnp.exp(cum_c)], axis=0), expand, precision=HIGH, preferred_element_type=F32
        )
        expd[cols, :] = both[blk:, :]
        wexps.append(both[:blk, :])
        cum_rs.append(cum_r)
        cum_cs.append(cum_c)
        st_rs.append(st_r)

    @pl.when(me > 0)
    def _():
        halo().wait_recv()
        ext[0:raw0, :] = hrecv[...].astype(F32)

    @pl.when(me == 0)
    def _():
        ext[0:raw0, :] = jnp.zeros((raw0, ext.shape[1]), F32)

    width = taps_v.shape[0]
    for b in range(blocks):
        for taps, lo, hi in ((taps_v, 0, cw), (taps_k, cw, cw + st), (taps_r, cw + st, cw + 2 * st)):
            total = jnp.zeros((blk, hi - lo), F32)
            for k in range(width):
                o = b * blk + raw0 - (width - 1) + k
                total = total + taps[k : k + 1, :] * ext[o : o + blk, cw + lo : cw + hi]
            conv[b * blk : (b + 1) * blk, lo:hi] = (total * jax.nn.sigmoid(total)).astype(BF)

    run = jnp.zeros((st, cw), F32)
    dec = jnp.ones((1, cw), F32)
    pres, offs = [], []
    for b in range(blocks):
        rows = slice(b * blk, (b + 1) * blk)
        key_t = bt(eye_st, conv[rows, cw : cw + st]).astype(BF)
        sv = conv[rows, 0:cw].astype(F32) * wexps[b]
        top, low = halves(sv)
        new = jnp.dot(key_t, top, preferred_element_type=F32) + jnp.dot(key_t, low, preferred_element_type=F32)
        bd = expd[(b + 1) * blk - 1 : (b + 1) * blk, :]
        pres.append(run)
        offs.append(dec)
        run = run * bd + new
        dec = dec * bd

    in_s = jnp.zeros((st, cw), F32)
    in_d = jnp.ones((1, cw), F32)
    rounds = [1 << k for k in range(S.bit_length() - 1)]

    def inner(b):
        rows = slice(b * blk, (b + 1) * blk)
        g = bt(conv[rows, cw + st :], conv[rows, cw : cw + st])
        for h in range(cw // hd):
            gap = jnp.where(lower, cum_cs[b][:, h : h + 1] - cum_rs[b][h : h + 1, :], -jnp.inf)
            wm = g * jnp.exp(gap) * st_rs[b][h : h + 1, :]
            top, low = halves(wm)
            v = conv[rows, h * hd : (h + 1) * hd]
            scan[rows, h * hd : (h + 1) * hd] = jnp.dot(top, v, preferred_element_type=F32) + jnp.dot(
                low, v, preferred_element_type=F32
            )

    window = lax.shift_left(jnp.int32(2), tp)
    back = (
        lax.broadcasted_iota(jnp.int32, (blk, blk + raw0), 0)
        + raw0
        - lax.broadcasted_iota(jnp.int32, (blk, blk + raw0), 1)
    )
    band = jnp.where((back >= 0) & (back < window), 1.0, 0.0).astype(BF)

    def pool(b):
        rows = slice(b * blk, (b + 1) * blk)
        sums = jnp.dot(band, ext[b * blk : (b + 1) * blk + raw0, 0:cw].astype(BF), preferred_element_type=F32)
        pos = (me * n + b * blk + lax.broadcasted_iota(jnp.int32, (blk, cw), 0)).astype(F32)
        counts = jnp.minimum(pos + 1.0, window.astype(F32))
        pooled = (sums / counts - ext[b * blk + raw0 : (b + 1) * blk + raw0, 0:cw]).astype(BF)
        brow[rows, 0:cw] = (jnp.dot(pooled, mix[0], preferred_element_type=F32) * scale[...]).astype(BF)

    work = [functools.partial(inner, b) for b in range(blocks)] + [functools.partial(pool, b) for b in range(blocks)]
    share = -(-len(work) // len(rounds))
    o_left = [(op, 1), (oq, even[0])] + [(op, m) for m in early_first(S)] + [(oq, m) for m in even[1:]]
    o_step = -(-len(o_left) // len(rounds))
    o_rest = [(op, m) for m in masks if (op, m) not in o_left] + [(oq, m) for m in odd]

    def take_o(count):
        for stream, mask in o_left[:count]:
            stream.got(mask)
        del o_left[:count]

    for r, bit in enumerate(rounds):
        xs[r, 0:st, :] = run
        xs[r, st:, :] = jnp.broadcast_to(dec, (xs.shape[1] - st, cw))
        send(xs.at[r], xr.at[r], x_ss.at[r], x_rs.at[r], sp=flip(me, bit))
        for f in work[r * share : (r + 1) * share]:
            f()
        take_o(o_step)
        remote(xs.at[r], xr.at[r], x_ss.at[r], x_rs.at[r], sp=flip(me, bit)).wait_recv()
        other, odec = xr[r, 0:st, :], xr[r, st : st + 1, :]
        later = lax.rem(lax.div(me, bit), 2) == 1
        in_s = jnp.where(later, other * in_d + in_s, in_s)
        in_d = jnp.where(later, odec * in_d, in_d)
        run = jnp.where(later, other * dec + run, run * odec + other)
        dec = dec * odec

    for b in range(blocks):
        rows = slice(b * blk, (b + 1) * blk)
        top, low = halves(pres[b] + offs[b] * in_s)
        rd = conv[rows, cw + st :]
        carried = jnp.dot(rd, top, preferred_element_type=F32) + jnp.dot(rd, low, preferred_element_type=F32)
        y = scan[rows, :] + carried * expd[rows, :] + skips * conv[rows, 0:cw].astype(F32)
        gt = acc[rows, cw : 2 * cw].astype(BF).astype(F32)
        gated = y * (gt * jax.nn.sigmoid(gt))
        ssend[:, rows] = bt(jnp.ones((8, cw), F32), gated * gated, precision=HIGH)
        brow[rows, cw:] = (gated * sgain[...]).astype(BF)
    for k in range(1, T):
        send(ssend, srecv.at[k - 1], q_ss.at[k - 1], q_rs.at[k - 1], tp=flip(tp, k))
    take_o(len(o_left))
    for stream, mask in o_rest:
        stream.got(mask)
    for k in range(1, T):
        remote(ssend, srecv.at[k - 1], q_ss.at[k - 1], q_rs.at[k - 1], tp=flip(tp, k)).wait_recv()
    sq = ssend[...]
    for k in range(1, T):
        sq = sq + srecv[k - 1]
    rs_row = lax.rsqrt(sq / (cw * T) + EPSILON)
    rs_cols = [bt(eye, rs_row[:, b * blk : (b + 1) * blk], precision=HIGH)[:, 0:1] for b in range(blocks)]
    wide = S // T
    oc = obuf.shape[2]
    parts = 4
    pr = n // parts

    def product(t, part, store):
        rows = slice(part * pr, (part + 1) * pr)
        rs = jnp.concatenate(rs_cols[part * blocks // parts : (part + 1) * blocks // parts], axis=0)
        for j in range(wide):
            i = t * wide + j
            p = jnp.dot(brow[rows, 0:cw], obuf[i, 0:cw, :], preferred_element_type=F32)
            p = p + rs * jnp.dot(brow[rows, cw:], obuf[i, cw:, :], preferred_element_type=F32)
            store(rows, slice(j * oc, (j + 1) * oc), p)

    def into(ref, *lead):
        def store(rows, cols, p):
            ref[lead + (rows, cols)] = p.astype(ref.dtype)
        return store

    near = flip(tp, 1)

    def near_copy(k, part):
        rows = pl.ds(part * pr, pr)
        i = k * parts + part
        return remote(psend.at[k, rows], precv.at[k, rows], p_ss.at[i], p_rs.at[i], tp=near)

    def far_copy(part):
        rows = pl.ds(part * pr, pr)
        return remote(qsend.at[rows], qrecv.at[rows], r_ss.at[part], r_rs.at[part], tp=flip(tp, 2))

    for part in range(parts + 1):
        if part < parts:
            product(flip(tp, 3), part, into(psend, 0))
            near_copy(0, part).start()
        if part > 0:
            rows = slice((part - 1) * pr, part * pr)
            product(flip(tp, 2), part - 1, into(pown))
            near_copy(0, part - 1).wait_recv()
            qsend[rows, :] = (pown[rows, :] + precv[0, rows, :]).astype(BF)
            far_copy(part - 1).start()
    for part in range(parts):
        product(near, part, into(psend, 1))
        near_copy(1, part).start()
    for part in range(parts):
        product(tp, part, into(pown))
    for part in range(parts):
        rows = slice(part * pr, (part + 1) * pr)
        near_copy(1, part).wait_recv()
        far_copy(part).wait_recv()
        out[rows, :] = (pown[rows, :] + precv[1, rows, :] + qrecv[rows, :].astype(F32)).astype(out.dtype)

    for c in started:
        c.wait_send()
    for part in range(parts):
        near_copy(0, part).wait_send()
        near_copy(1, part).wait_send()
        far_copy(part).wait_send()

    @pl.when(me < S - 1)
    def _():
        halo().wait_send()


def fits(S, T, shapes):
    n, da = shapes[0]
    kd, cw = shapes[2]
    st = shapes[5][1]
    oc = shapes[18][1]
    heads = shapes[7][1]
    return (
        T == 4 == POOL_GROUPS and S >= T and S & (S - 1) == 0 and S <= 16 and st == SSM_STATE
        and cw == heads * SSM_STATE and n % (4 * SCAN_BLOCK) == 0
        and -(-kd // 96) * 2 * cw % kd == 0 and oc % 128 == 0 and kd % 128 == 0 and da % kd == 0
        and n % (2 * SCAN_BLOCK) == 0 and cw % 128 == 0 and oc * S == da * T
    )


def fused(
    S, T, activations, norm_gain, pool_weight, gate_weight, value_weight, key_weight, read_weight,
    step_weight, pool_mix, pool_scale, taps_value, taps_key, taps_read, step_bias, decay_log,
    decay_extra, skip_scale, state_gain, out_pool_weight, out_state_weight,
):
    n, da = activations.shape
    kd, cw = pool_weight.shape
    st = key_weight.shape[1]
    heads = step_weight.shape[1]
    oc = out_pool_weight.shape[1]
    hp = 16
    args = (
        activations, norm_gain[None, :], pool_weight, gate_weight, value_weight, key_weight.T, read_weight.T,
        step_weight.T, pool_mix, pool_scale[None, :], taps_value, taps_key, taps_read, step_bias[None, :], decay_log[None, :],
        decay_extra.T, skip_scale[None, :], state_gain[None, :],
        out_pool_weight, out_state_weight,
    )
    ncol = 3 * cw + 2 * st
    ccol = ncol - cw
    V = pltpu.VMEM
    D = pltpu.SemaphoreType.DMA
    R = S.bit_length() - 1
    scratch = [
        V((S, kd, ncol), BF), V((S, hp, kd), BF), V((S, 2 * cw, oc), BF), V((T, n + 16, da), BF),
        V((S, n, kd), BF), V((n, ncol), F32), V((hp, n), F32), V((n + 16, ccol), F32),
        V((n, cw + 2 * st), BF), V((16, ccol), BF), V((16, ccol), BF), V((n, cw), F32),
        V((R, st + 8, cw), F32), V((R, st + 8, cw), F32), V((8, n), F32), V((T - 1, 8, n), F32),
        V((n, 2 * cw), BF), V((2, n, da), F32), V((2, n, da), F32), V((n, da), F32),
        V((n, da), BF), V((n, da), BF), V((n, cw), F32),
        D((2 * S,)), D((2 * S,)), D((S,)), D((S,)), D((2 * S,)), D((2 * S,)), D((T,)), D((T,)), D, D,
        D((R,)), D((R,)), D((T,)), D((T,)), D((8,)), D((8,)), D((4,)), D((4,)),
    ]
    return pl.pallas_call(
        functools.partial(mixer_kernel, S, T),
        out_shape=jax.ShapeDtypeStruct((n, da), BF),
        in_specs=[pl.BlockSpec(memory_space=pltpu.VMEM)] * len(args),
        out_specs=pl.BlockSpec(memory_space=pltpu.VMEM),
        scratch_shapes=scratch,
        compiler_params=pltpu.CompilerParams(
            collective_id=0, has_side_effects=True, vmem_limit_bytes=60 * 1024 * 1024
        ),
    )(*args)


def solution(mesh):
    placed = (
        P("sp", "tp"),
        P("tp"),
        P("sp", "tp"),
        P("sp", "tp"),
        P("sp", "tp"),
        P("sp", "tp"),
        P("sp", "tp"),
        P("sp", "tp"),
        P("tp", None, None),
        P("tp"),
        P(None, "tp"),
        P(None, "tp"),
        P(None, "tp"),
        P("tp"),
        P("tp"),
        P("sp", "tp"),
        P("tp"),
        P("tp"),
        P("tp", "sp"),
        P("tp", "sp"),
    )
    S, T = mesh.shape["sp"], mesh.shape["tp"]

    def chosen(*args):
        if fits(S, T, [a.shape for a in args]):
            return fused(S, T, *args)
        return local(*args)

    return jax.shard_map(
        chosen, mesh=mesh, in_specs=placed, out_specs=P("sp", "tp"), check_vma=False
    )
```
